128 devices in a mesh: sp: 64 (over z, y, x), tp: 2 (over core).
Axes of the slice: x: 4, y: 4, z: 4, core: 2. Of those that a mesh axis runs over, the one named last changes fastest.
Arguments:
- mixer_output: bfloat16 [8192, 2048], P('sp'), may hold values from -6 to 6
- layer_cotangent: bfloat16 [8192, 2048], P('sp'), may hold values from -16 to 16
- expert_choice: int32 [8192, 2], P('sp'), may hold values from 0 to 63, all different within a row; in each aligned block of 128 rows (0 to 127, 128 to 255, ...) at most 8 rows name the same one
- route_weight: float32 [8192, 2], P('sp'), may hold values from 0.1 to 0.9
- gate_pre: bfloat16 [64, 512, 1024], P('sp', None, 'tp'), may hold values from -15 to 15
- up_pre: bfloat16 [64, 512, 1024], P('sp', None, 'tp'), may hold values from -15 to 15
- w_gate: bfloat16 [64, 2048, 1024], P('sp', None, 'tp'), may hold values from -0.125 to 0.125
- w_up: bfloat16 [64, 2048, 1024], P('sp', None, 'tp'), may hold values from -0.125 to 0.125
- w_down: bfloat16 [64, 1024, 2048], P('sp', 'tp'), may hold values from -0.1875 to 0.1875
- w_out: bfloat16 [2048, 2048], P('tp'), may hold values from -0.125 to 0.125
- norm_gain: bfloat16 [2048], P('tp'), may hold values from 0.099609375 to 1.8984375
- scan_in: bfloat16 [8192, 2048], P('sp', 'tp'), may hold values from -6 to 6
- gate_in: bfloat16 [8192, 2048], P('sp', 'tp'), may hold values from -9 to 9
- b_proj: bfloat16 [8192, 1024], P('sp', 'tp'), may hold values from -1.796875 to 1.796875
- c_proj: bfloat16 [8192, 1024], P('sp', 'tp'), may hold values from -1.796875 to 1.796875
- log_decay: float32 [8192, 32], P('sp', 'tp'), may hold values from -3 to 0
- entry_state: float32 [64, 32, 64, 128], P('sp', 'tp'), may hold values from -24 to 24
Outputs:
- grad_w_gate: bfloat16 [64, 2048, 1024], P('sp', None, 'tp')
- grad_w_up: bfloat16 [64, 2048, 1024], P('sp', None, 'tp')
- grad_w_down: bfloat16 [64, 1024, 2048], P('sp', 'tp')
- grad_out_proj: float32 [2048, 2048], P('sp', 'tp')
- grad_scan_in: bfloat16 [8192, 2048], P('sp', 'tp')
- grad_gate_in: bfloat16 [8192, 2048], P('sp', 'tp')
- grad_b_proj: bfloat16 [8192, 1024], P('sp', 'tp')
- grad_c_proj: bfloat16 [8192, 1024], P('sp', 'tp')
- grad_log_decay: float32 [8192, 32], P('sp', 'tp')
The draws below stay inside these ranges and needn't reach their ends.
Inputs may be any that keep to these rules, and one draw needn't show every extreme that they name: `expert_choice`: in the 128 rows of one device no expert is named more than 8 times, a bound that some blocks reach; the 2 entries of a row differ.
All inputs are finite; a program needn't handle non-finite values.
Results may differ from the reference program's by a relative error of at most 0.012.
Values may be sent and summed in bfloat16 or wider, within the bound.
A program may use at most 192 MiB of HBM per device.

```python
import math
from functools import partial
import jax
import jax.numpy as jnp
import numpy as np
from jax import lax

D = 2048
MIXER_HEADS = 32
HEAD_DIM = 64
GROUPS = 8
STATE = 128
FF = 1024
TOPK = 2
TOK_DEV = 128
SEQUENCE_TOKENS = 8192
EXPERTS = 64
INNER = 2048
CAP = 8
EXPERT_ROWS = 512
N_SP = 64
N_TP = 2


def draw_log_decay(key, part):
    random_keys_split = jax.random.split(key, 7)
    fast_share = 0.5
    is_fast = jax.random.uniform(random_keys_split[0], (MIXER_HEADS,)) < fast_share
    fast_rate = jax.random.uniform(random_keys_split[1], (MIXER_HEADS,), minval=1.0 / 100.0, maxval=1.0 / 30.0)
    slow_rate = jax.random.uniform(random_keys_split[2], (MIXER_HEADS,), minval=0.05, maxval=0.3) * math.log(10.0) / SEQUENCE_TOKENS
    base_rate = jnp.where(is_fast, fast_rate, slow_rate)
    block_count = SEQUENCE_TOKENS // TOK_DEV
    block_factor = jnp.exp(jax.random.uniform(random_keys_split[3], (block_count, 1, MIXER_HEADS), minval=math.log(0.5), maxval=math.log(2.0)))
    token_factor = jnp.exp(jax.random.uniform(random_keys_split[4], (block_count, TOK_DEV, MIXER_HEADS), minval=math.log(0.5), maxval=math.log(2.0)))
    decay_rate_table = (base_rate[None, None, :] * block_factor * token_factor).reshape(SEQUENCE_TOKENS, MIXER_HEADS)
    spike_positions = jax.random.randint(random_keys_split[5], (3, MIXER_HEADS), 0, SEQUENCE_TOKENS)
    spike_length = jnp.log(jax.random.uniform(random_keys_split[6], (3, MIXER_HEADS), minval=0.5, maxval=0.8))
    token_locations = jnp.arange(SEQUENCE_TOKENS)[:, None]
    spike_events = jnp.zeros((SEQUENCE_TOKENS, MIXER_HEADS), jnp.float32)
    for event_count in range(3):
        spike_events = spike_events + jnp.where(token_locations == spike_positions[event_count][None, :], spike_length[event_count][None, :], 0.0)
    return (spike_events - decay_rate_table).astype(jnp.float32)


def raised(drawn, rng, source, target, parts, factor):
    owner, partner = [(jnp.arange(drawn.shape[dim]) // (drawn.shape[dim] // parts)).reshape([-1 if axis == dim else 1 for axis in range(drawn.ndim)]) for dim in (source, target)]
    chosen = jax.random.permutation(rng, parts)[partner]
    strong = (owner == chosen) | (owner == (partner + parts // 2) % parts)
    return jnp.where(strong, factor * drawn, drawn)


def steps_of(key, extent, shards, low, top_value):
    loudness, own = 1.0, jax.random.fold_in(key, 6)
    for dim, blocks in shards:
        draws = jnp.exp(jax.random.uniform(jax.random.fold_in(own, dim), (blocks,), jnp.float32, low / len(shards), top_value / len(shards)))
        loudness = loudness * jnp.repeat(draws, extent[dim] // blocks).reshape([-1 if axis == dim else 1 for axis in range(len(extent))])
    return loudness


def shared_out(own_key, own, number, rows, count, top, most, lean):
    ranking = jax.random.permutation(own_key, count)
    crowded, usual = load_shares(count, rows * top, most, lean, True), load_shares(count, rows * top, most, lean, False)
    places = jnp.arange(count)

    def named(sizes, offset_by):
        used = int((sizes > 0).sum())
        fixed = max(1, used // 4)
        shifted = fixed + (places - fixed + offset_by * (used - fixed)) % max(1, count - fixed)
        return jnp.zeros((count,), jnp.int32).at[ranking[jnp.where(places < fixed, places, shifted)]].set(jnp.asarray(sizes, jnp.int32))

    sizes = jnp.where(number % 4 == 0, named(crowded, number // 4), named(usual, number - number // 4 - 1))
    mixed = jax.random.permutation(jax.random.fold_in(own, 3), count)
    giver, sink = mixed[0:count // 2 * 2:2], mixed[1:count // 2 * 2:2]
    room = jnp.minimum(sizes[giver] - 1, most - sizes[sink]) // 2
    room = jnp.where((giver == ranking[0]) | (sink == ranking[0]) | (sizes[sink] == 0), 0, jnp.maximum(room, 0))
    shifted = jax.random.randint(jax.random.fold_in(own, 4), (count // 2,), 0, 1 << 20) % (room + 1)
    sizes = sizes.at[giver].add(-shifted).at[sink].add(shifted)
    items = jnp.searchsorted(jnp.cumsum(sizes), jnp.arange(rows * top), side="right").astype(jnp.int32)
    listing = items.reshape(top, rows).T
    listing = listing[jax.random.permutation(jax.random.fold_in(own, 1), rows)]
    offset_by = jax.random.randint(jax.random.fold_in(own, 2), (rows, 1), 0, top)
    return jnp.take_along_axis(listing, (jnp.arange(top)[None, :] + offset_by) % top, axis=1)


def load_shares(number_of, total, most, skew, full):
    portions = [(1 << 20) // math.isqrt(grade ** skew) + 1 for grade in range(1, number_of + 1)]
    largest = most if full else min(most, max(-(-total // number_of), total * portions[0] // sum(portions)))
    least = 1 if total - largest >= number_of - 1 else 0
    given, surplus = [largest] + [least] * (number_of - 1), total - largest - least * (number_of - 1)
    while surplus > 0:
        candidates = [i for i in range(1, number_of) if given[i] < largest] or [i for i in range(1, number_of) if given[i] < most]
        whole, remaining = sum([portions[i] for i in candidates]), surplus
        for i in candidates:
            extra = min(most - given[i], max(1, remaining * portions[i] // whole), surplus)
            given[i] = given[i] + extra
            surplus = surplus - extra
    return np.array(given)


def normal_values(stream_key, dims, deviation, reach, cuts=(), kind=jnp.bfloat16):
    drawn = deviation * jax.random.normal(stream_key, dims, jnp.float32)
    if cuts:
        drawn = drawn * steps_of(stream_key, dims, cuts, -0.22, 0.18)
    return jnp.clip(drawn, -reach, reach).astype(kind)


def bell_draw_with(own_key, extent, spread, bound, cuts, heavy, kind=jnp.bfloat16):
    values = spread * jax.random.normal(own_key, extent, jnp.float32)
    if cuts:
        values = values * steps_of(own_key, extent, cuts, -0.22, 0.18)
    return jnp.clip(raised(values, jax.random.fold_in(own_key, 3), *heavy), -bound, bound).astype(kind)


def setup_inputs(seed: int = 0) -> dict:
    streams_of = jax.random.split(jax.random.key(seed), 18)
    mixer_output = normal_values(streams_of[0], (SEQUENCE_TOKENS, D), 1.0, 6.0, ((0, 64),))
    layer_cotangent = bell_draw_with(streams_of[1], (SEQUENCE_TOKENS, D), 1.0, 16.0, ((0, 64),), (0, 1, 64, 4.0))
    expert_choice_keys = jax.random.split(jax.random.fold_in(streams_of[2], 1), SEQUENCE_TOKENS // TOK_DEV)
    expert_choice_turns = jax.random.permutation(jax.random.fold_in(streams_of[2], 3), SEQUENCE_TOKENS // TOK_DEV)
    expert_choice = jax.vmap(lambda own, number: shared_out(jax.random.fold_in(streams_of[2], 2), own, number, TOK_DEV, EXPERTS, TOPK, CAP, 1))(expert_choice_keys, expert_choice_turns).reshape((SEQUENCE_TOKENS, TOPK))
    route_weight = jnp.clip(0.1 + 0.79999997 * jax.random.uniform(streams_of[3], (SEQUENCE_TOKENS, TOPK), jnp.float32) ** steps_of(streams_of[3], (SEQUENCE_TOKENS, TOPK), ((0, 64),), -0.2, 0.2), 0.1, 0.9)
    gate_pre = normal_values(streams_of[4], (EXPERTS, EXPERT_ROWS, FF), 3.0, 15.0, ((0, 64), (2, 2)))
    up_pre = normal_values(streams_of[5], (EXPERTS, EXPERT_ROWS, FF), 3.0, 15.0, ((0, 64), (2, 2)))
    w_gate = normal_values(streams_of[6], (EXPERTS, D, FF), D ** -0.5, 0.125, ((0, 64), (2, 2)))
    w_up = normal_values(streams_of[7], (EXPERTS, D, FF), D ** -0.5, 0.125, ((0, 64), (2, 2)))
    w_down = normal_values(streams_of[8], (EXPERTS, FF, D), FF ** -0.5, 0.1875, ((0, 64), (1, 2)))
    w_out = normal_values(streams_of[9], (INNER, D), INNER ** -0.5, 0.125, ((0, 2),))
    norm_gain = jnp.clip(1.0 + 0.18 * jax.random.normal(streams_of[10], (INNER,), jnp.float32), 0.099609375, 1.8984375).astype(jnp.bfloat16)
    scan_in = normal_values(streams_of[11], (SEQUENCE_TOKENS, INNER), 1.0, 6.0, ((0, 64), (1, 2)))
    gate_in = normal_values(streams_of[12], (SEQUENCE_TOKENS, INNER), 1.5, 9.0, ((0, 64), (1, 2)))
    b_proj = normal_values(streams_of[13], (SEQUENCE_TOKENS, GROUPS * STATE), 0.3, 1.796875, ((0, 64), (1, 2)))
    c_proj = normal_values(streams_of[14], (SEQUENCE_TOKENS, GROUPS * STATE), 0.3, 1.796875, ((0, 64), (1, 2)))
    log_decay = draw_log_decay(jax.random.fold_in(streams_of[17], 71), 0)
    entry_state = normal_values(streams_of[16], (N_SP, MIXER_HEADS, HEAD_DIM, STATE), 4.0, 24.0, ((0, 64), (1, 2)), jnp.float32)
    return {"mixer_output": mixer_output, "layer_cotangent": layer_cotangent, "expert_choice": expert_choice, "route_weight": route_weight, "gate_pre": gate_pre, "up_pre": up_pre, "w_gate": w_gate, "w_up": w_up, "w_down": w_down, "w_out": w_out, "norm_gain": norm_gain, "scan_in": scan_in, "gate_in": gate_in, "b_proj": b_proj, "c_proj": c_proj, "log_decay": log_decay, "entry_state": entry_state}


rms_epsilon = 1e-05
clamp_limit = 7.0
swish_alpha = 1.702

def slot_ranks(expert_ids, expert_count):
    targets = expert_ids.reshape(-1)
    one_hot = (targets[:, None] == jnp.arange(expert_count, dtype=jnp.int32)[None, :]).astype(jnp.int32)
    earlier = jnp.cumsum(one_hot, axis=0) - one_hot
    return (targets, lax.optimization_barrier(jnp.sum(earlier * one_hot, axis=1)).astype(jnp.int32))

def fill_slots(rows, targets, ranked):
    buffer = jnp.zeros((N_SP, CAP, rows.shape[1]), rows.dtype)
    return buffer.at[targets, ranked].set(rows)

def pick_rows(buffer, targets, ranked):
    return buffer[targets, ranked]

def expert_ref(inputs):
    hidden_rows, grad_rows, gate_value, up_value, gate_weight, up_weight, down_weight = inputs
    act_grad = jnp.dot(grad_rows, down_weight.T, preferred_element_type=jnp.float32)
    gate_full = gate_value.astype(jnp.float32)
    up_full = up_value.astype(jnp.float32)
    gate_clip = jnp.minimum(gate_full, clamp_limit)
    up_clip = jnp.clip(up_full, -clamp_limit, clamp_limit)
    sigmoid_gate = jax.nn.sigmoid(swish_alpha * gate_clip)
    swish_gate = gate_clip * sigmoid_gate
    active = ((up_clip + 1.0) * swish_gate).astype(jnp.bfloat16)
    up_grad = jnp.where((up_full > -clamp_limit) & (up_full < clamp_limit), act_grad * swish_gate, 0.0).astype(jnp.bfloat16)
    slope = sigmoid_gate + swish_alpha * gate_clip * sigmoid_gate * (1.0 - sigmoid_gate)
    gate_grad = jnp.where(gate_full < clamp_limit, act_grad * (up_clip + 1.0) * slope, 0.0).astype(jnp.bfloat16)
    down_wgrad = jnp.dot(active.T, grad_rows, preferred_element_type=jnp.float32).astype(jnp.bfloat16)
    gate_wgrad = jnp.dot(hidden_rows.T, gate_grad, preferred_element_type=jnp.float32).astype(jnp.bfloat16)
    up_wgrad = jnp.dot(hidden_rows.T, up_grad, preferred_element_type=jnp.float32).astype(jnp.bfloat16)
    row_count = gate_grad.shape[0]
    part_width = FF // N_TP
    gate_split = gate_grad.reshape(row_count, N_TP, part_width).astype(jnp.float32)
    up_split = up_grad.reshape(row_count, N_TP, part_width).astype(jnp.float32)
    gate_parts = gate_weight.reshape(D, N_TP, part_width).astype(jnp.float32)
    up_parts = up_weight.reshape(D, N_TP, part_width).astype(jnp.float32)
    partial_rows = jnp.einsum('rjf,djf->jrd', gate_split, gate_parts) + jnp.einsum('rjf,djf->jrd', up_split, up_parts)
    rounded = lax.optimization_barrier(partial_rows.astype(jnp.bfloat16))
    back_rows = lax.optimization_barrier(jnp.sum(rounded.astype(jnp.float32), axis=0)).astype(jnp.bfloat16)
    return (gate_wgrad, up_wgrad, down_wgrad, back_rows)

def block_step(carry, inputs, w_out, norm_gain):
    later_state, later_grad = carry
    scan_block, gate_block, b_block, c_block, decay_block, state_block, hidden_block = inputs
    length = scan_block.shape[0]
    per_group = MIXER_HEADS // GROUPS
    scan_heads = scan_block.reshape(length, MIXER_HEADS, HEAD_DIM).astype(jnp.float32)
    b_groups = b_block.reshape(length, GROUPS, STATE).astype(jnp.float32)
    c_groups = c_block.reshape(length, GROUPS, STATE).astype(jnp.float32)
    cumulative = jnp.cumsum(decay_block, axis=0)
    growth = jnp.exp(cumulative)
    tail_decay = jnp.exp(cumulative[-1][None, :] - cumulative)
    token_locations = jnp.arange(length)
    causal = token_locations[:, None] >= token_locations[None, :]
    log_gaps = cumulative.T[:, :, None] - cumulative.T[:, None, :]
    decay_mat = jnp.exp(jnp.where(causal[None], log_gaps, -jnp.inf))
    inner_prod = jnp.einsum('tgn,sgn->gts', c_groups, b_groups)
    mix_weights = (jnp.repeat(inner_prod, per_group, axis=0) * decay_mat).astype(jnp.bfloat16).astype(jnp.float32)
    state_groups = state_block.reshape(GROUPS, per_group, HEAD_DIM, STATE)
    y_inner = jnp.einsum('hts,shp->thp', mix_weights, scan_heads)
    y_carry = jnp.einsum('tgn,grpn->tgrp', c_groups, state_groups, precision=lax.Precision.HIGHEST).reshape(length, MIXER_HEADS, HEAD_DIM)
    scan_out = y_inner + y_carry * growth[:, :, None]
    gate_float = gate_block.astype(jnp.float32)
    gate_sig = jax.nn.sigmoid(gate_float)
    gate_silu = gate_float * gate_sig
    gated = scan_out.reshape(length, -1) * gate_silu
    grouped = gated.reshape(length, GROUPS, -1)
    inv_rms = lax.rsqrt(lax.optimization_barrier(jnp.mean(grouped * grouped, axis=-1, keepdims=True)) + rms_epsilon)
    unit = grouped * inv_rms
    gain_groups = norm_gain.astype(jnp.float32).reshape(GROUPS, -1)
    mixed = (unit * gain_groups).reshape(length, -1).astype(jnp.bfloat16)
    grad_mixed = jnp.dot(hidden_block, w_out.T, preferred_element_type=jnp.float32)
    grad_unit = grad_mixed.reshape(length, GROUPS, -1) * gain_groups
    grad_grouped = inv_rms * (grad_unit - unit * lax.optimization_barrier(jnp.mean(grad_unit * unit, axis=-1, keepdims=True)))
    grad_gated = grad_grouped.reshape(length, -1)
    grad_gate = (grad_gated * scan_out.reshape(length, -1) * gate_sig * (1.0 + gate_float * (1.0 - gate_sig))).astype(jnp.bfloat16)
    grad_y = (grad_gated * gate_silu).reshape(length, MIXER_HEADS, HEAD_DIM)
    grad_y_b = grad_y.astype(jnp.bfloat16).astype(jnp.float32)
    grad_x_inner = jnp.einsum('hts,thp->shp', mix_weights, grad_y_b)
    grad_weights = (jnp.einsum('thp,shp->hts', grad_y_b, scan_heads) * decay_mat).reshape(GROUPS, per_group, length, length).sum(axis=1)
    grad_weights = grad_weights.astype(jnp.bfloat16).astype(jnp.float32)
    grad_c_inner = jnp.einsum('gts,sgn->tgn', grad_weights, b_groups)
    grad_b_inner = jnp.einsum('gts,tgn->sgn', grad_weights, c_groups)
    grown_grads = (grad_y * growth[:, :, None]).reshape(length, GROUPS, per_group, HEAD_DIM)
    grad_c_carry = jnp.einsum('tgrp,grpn->tgn', grown_grads, state_groups, precision=lax.Precision.HIGHEST)
    block_state = jnp.einsum('tgrp,tgn->grpn', grown_grads, c_groups, precision=lax.Precision.HIGHEST).reshape(MIXER_HEADS, HEAD_DIM, STATE)
    later_groups = later_state.reshape(GROUPS, per_group, HEAD_DIM, STATE)
    grad_x_carry = jnp.einsum('sgn,grpn->sgrp', b_groups, later_groups, precision=lax.Precision.HIGHEST).reshape(length, MIXER_HEADS, HEAD_DIM)
    grad_x = grad_x_inner + grad_x_carry * tail_decay[:, :, None]
    x_tail = (scan_heads * tail_decay[:, :, None]).reshape(length, GROUPS, per_group, HEAD_DIM)
    grad_b_carry = jnp.einsum('sgrp,grpn->sgn', x_tail, later_groups, precision=lax.Precision.HIGHEST)
    grad_a = lax.optimization_barrier(jnp.sum(grad_y * scan_out, axis=2)) - lax.optimization_barrier(jnp.sum(scan_heads * grad_x, axis=2))
    grad_decay = jnp.flip(jnp.cumsum(jnp.flip(grad_a, 0), axis=0), 0) + later_grad[None, :]
    new_state = block_state + jnp.exp(cumulative[-1])[:, None, None] * later_state
    new_grad = later_grad + lax.optimization_barrier(jnp.sum(grad_a, axis=0))
    outputs = (grad_x.reshape(length, -1).astype(jnp.bfloat16), grad_gate, (grad_b_inner + grad_b_carry).reshape(length, -1).astype(jnp.bfloat16), (grad_c_inner + grad_c_carry).reshape(length, -1).astype(jnp.bfloat16), grad_decay, mixed)
    return ((new_state, new_grad), outputs)

def reference(mixer_output, layer_cotangent, expert_choice, route_weight, gate_pre, up_pre, w_gate, w_up, w_down, w_out, norm_gain, scan_in, gate_in, b_proj, c_proj, log_decay, entry_state):
    id_blocks = expert_choice.reshape(N_SP, TOK_DEV, TOPK)
    targets, ranked = jax.vmap(partial(slot_ranks, expert_count=N_SP))(id_blocks)
    token_of = jnp.arange(SEQUENCE_TOKENS * TOPK, dtype=jnp.int32) // TOPK
    hidden_rows = mixer_output[token_of].reshape(N_SP, TOK_DEV * TOPK, D)
    grad_rows = (route_weight.reshape(-1)[:, None] * layer_cotangent[token_of].astype(jnp.float32)).astype(jnp.bfloat16)
    grad_rows = grad_rows.reshape(N_SP, TOK_DEV * TOPK, D)
    send_hidden = jax.vmap(fill_slots)(hidden_rows, targets, ranked)
    send_grads = jax.vmap(fill_slots)(grad_rows, targets, ranked)
    recv_hidden = jnp.transpose(send_hidden, (1, 0, 2, 3)).reshape(N_SP, N_SP * CAP, D)
    recv_grads = jnp.transpose(send_grads, (1, 0, 2, 3)).reshape(N_SP, N_SP * CAP, D)
    gate_wgrad, up_wgrad, down_wgrad, back_rows = lax.map(expert_ref, (recv_hidden, recv_grads, gate_pre, up_pre, w_gate, w_up, w_down))
    returned = jnp.transpose(back_rows.reshape(N_SP, N_SP, CAP, D), (1, 0, 2, 3))
    picked = jax.vmap(pick_rows)(returned, targets, ranked)
    moe_terms = picked.astype(jnp.float32).reshape(SEQUENCE_TOKENS, TOPK, D).sum(axis=1)
    grad_hidden = (layer_cotangent.astype(jnp.float32) + moe_terms).astype(jnp.bfloat16)

    def blocks_of(array):
        return array.reshape((N_SP, TOK_DEV) + array.shape[1:])
    initial = (jnp.zeros((MIXER_HEADS, HEAD_DIM, STATE), jnp.float32), jnp.zeros((MIXER_HEADS,), jnp.float32))
    stepper = partial(block_step, w_out=w_out, norm_gain=norm_gain)
    block_inputs = (blocks_of(scan_in), blocks_of(gate_in), blocks_of(b_proj), blocks_of(c_proj), blocks_of(log_decay), entry_state, blocks_of(grad_hidden))
    results = lax.scan(stepper, initial, block_inputs, reverse=True)[1]
    grad_scan, grad_gate, grad_b, grad_c, grad_decay, mixed = [item.reshape((SEQUENCE_TOKENS,) + item.shape[2:]) for item in results]
    grad_out_proj = jnp.dot(grad_hidden.T, mixed, preferred_element_type=jnp.float32)
    return (gate_wgrad, up_wgrad, down_wgrad, grad_out_proj, grad_scan, grad_gate, grad_b, grad_c, grad_decay)
```

```python
import jax
import jax.numpy as jnp
from jax import lax
from jax.sharding import Mesh
from jax.sharding import PartitionSpec as P

HEAD_DIM = 64
STATE = 128
SP = ("sp_0", "sp_1", "sp_2")


rms_epsilon = 1e-05
clamp_limit = 7.0
swish_alpha = 1.702


def expert_side(hidden_rows, grad_rows, gate_value, up_value, gate_weight, up_weight, down_weight):
    act_grad = jnp.einsum("rd,fd->rf", grad_rows, down_weight, preferred_element_type=jnp.float32)
    gate_full = gate_value.astype(jnp.float32)
    up_full = up_value.astype(jnp.float32)
    gate_clip = jnp.minimum(gate_full, clamp_limit)
    up_clip = jnp.clip(up_full, -clamp_limit, clamp_limit)
    sigmoid_gate = jax.nn.sigmoid(swish_alpha * gate_clip)
    swish_gate = gate_clip * sigmoid_gate
    active = ((up_clip + 1.0) * swish_gate).astype(jnp.bfloat16)
    up_grad = jnp.where(
        (up_full > -clamp_limit) & (up_full < clamp_limit), act_grad * swish_gate, 0.0
    ).astype(jnp.bfloat16)
    slope = sigmoid_gate + swish_alpha * gate_clip * sigmoid_gate * (1.0 - sigmoid_gate)
    gate_grad = jnp.where(gate_full < clamp_limit, act_grad * (up_clip + 1.0) * slope, 0.0).astype(
        jnp.bfloat16
    )
    down_wgrad = jnp.einsum(
        "rf,rd->fd", active, grad_rows, preferred_element_type=jnp.float32
    ).astype(jnp.bfloat16)
    gate_wgrad = jnp.einsum(
        "rd,rf->df", hidden_rows, gate_grad, preferred_element_type=jnp.float32
    ).astype(jnp.bfloat16)
    up_wgrad = jnp.einsum(
        "rd,rf->df", hidden_rows, up_grad, preferred_element_type=jnp.float32
    ).astype(jnp.bfloat16)
    partial_rows = jnp.einsum(
        "rf,df->rd", gate_grad, gate_weight, preferred_element_type=jnp.float32
    )
    partial_rows = partial_rows + jnp.einsum(
        "rf,df->rd", up_grad, up_weight, preferred_element_type=jnp.float32
    )
    return (gate_wgrad, up_wgrad, down_wgrad, partial_rows)


def slot_rows(expert_choice, expert_count, capacity):
    choice = expert_choice.T
    tokens = choice.shape[1]
    experts = lax.broadcasted_iota(jnp.int32, (expert_count, tokens), 0)
    hots = [(experts == choice[k][None, :]) for k in range(choice.shape[0])]
    named = sum(h.astype(jnp.bfloat16) for h in hots)
    before = (
        lax.broadcasted_iota(jnp.int32, (tokens, tokens), 0)
        < lax.broadcasted_iota(jnp.int32, (tokens, tokens), 1)
    ).astype(jnp.bfloat16)
    earlier = jnp.dot(named, before, preferred_element_type=jnp.float32)
    places = lax.broadcasted_iota(jnp.int32, (expert_count * capacity, tokens), 0)
    out = []
    for k, hot in enumerate(hots):
        rank = jnp.sum(jnp.where(hot, earlier, 0.0), axis=0).astype(jnp.int32)
        slot = choice[k] * capacity + rank
        out.append((places == slot[None, :]).astype(jnp.bfloat16))
    return out


def body(
    mixer_output,
    layer_cotangent,
    expert_choice,
    route_weight,
    gate_pre,
    up_pre,
    w_gate,
    w_up,
    w_down,
    w_out,
    norm_gain,
    scan_in,
    gate_in,
    b_proj,
    c_proj,
    log_decay,
    entry_state,
):
    f32, bf16 = jnp.float32, jnp.bfloat16
    expert_count = lax.axis_size(SP)
    sp = lax.axis_index(SP)
    tokens_here, model_width = mixer_output.shape
    capacity = gate_pre.shape[1] // expert_count
    half_width = model_width // lax.axis_size("tp")
    half_start = lax.axis_index("tp") * half_width
    mixer_half = lax.dynamic_slice_in_dim(mixer_output, half_start, half_width, 1)
    cotangent_half = lax.dynamic_slice_in_dim(layer_cotangent, half_start, half_width, 1)
    hot0, hot1 = slot_rows(expert_choice, expert_count, capacity)
    hot_any = hot0 + hot1
    cot_f = cotangent_half.astype(f32)
    rows0 = (route_weight[:, 0:1] * cot_f).astype(bf16)
    rows1 = (route_weight[:, 1:2] * cot_f).astype(bf16)
    send_grads = jnp.dot(
        jnp.concatenate([hot0, hot1], axis=1),
        jnp.concatenate([rows0, rows1], axis=0),
        preferred_element_type=f32,
    ).astype(bf16)
    send_hidden = jnp.dot(hot_any, mixer_half, preferred_element_type=f32).astype(bf16)

    def exchanged(rows):
        return lax.all_to_all(
            rows.reshape(expert_count, capacity, -1), SP, 0, 0, tiled=True
        ).reshape(expert_count * capacity, -1)

    both = jnp.concatenate(
        [
            send_grads.reshape(expert_count, capacity, -1),
            send_hidden.reshape(expert_count, capacity, -1),
        ],
        axis=1,
    )
    came = lax.all_to_all(both, SP, 0, 0, tiled=True)
    came = jnp.concatenate(
        [
            came[:, :capacity].reshape(-1, half_width),
            came[:, capacity:].reshape(-1, half_width),
        ],
        axis=0,
    )
    came = lax.all_gather(came, "tp", axis=1, tiled=True)
    recv_grads, recv_hidden = jnp.split(came, 2, axis=0)
    gate_wgrad, up_wgrad, down_wgrad, partial_rows = expert_side(
        recv_hidden, recv_grads, gate_pre[0], up_pre[0], w_gate[0], w_up[0], w_down[0]
    )
    pieces = partial_rows.astype(bf16).reshape(-1, 2, half_width)
    pieces = lax.all_to_all(pieces.transpose(1, 0, 2), "tp", 0, 0, tiled=True)
    summed = (pieces[0].astype(f32) + pieces[1].astype(f32)).astype(bf16)
    returned = exchanged(summed)
    moe_half = lax.dot_general(
        hot_any, returned, (((0,), (0,)), ((), ())), preferred_element_type=f32
    )
    hidden_half = (cot_f + moe_half).astype(bf16)
    grad_hidden = lax.all_gather(hidden_half, "tp", axis=1, tiled=True)

    head_count = log_decay.shape[1]
    group_count = b_proj.shape[1] // STATE
    per_group = head_count // group_count
    scan_heads = scan_in.reshape(tokens_here, head_count, HEAD_DIM)
    b_groups = b_proj.reshape(tokens_here, group_count, STATE)
    c_groups = c_proj.reshape(tokens_here, group_count, STATE)
    x_float = scan_heads.astype(f32)
    b_float = b_groups.astype(f32)
    c_float = c_groups.astype(f32)
    cumulative = jnp.cumsum(log_decay, axis=0)
    growth = jnp.exp(cumulative)
    tail_decay = jnp.exp(cumulative[-1][None, :] - cumulative)
    token_locations = jnp.arange(tokens_here)
    causal = token_locations[:, None] >= token_locations[None, :]
    log_gaps = cumulative.T[:, :, None] - cumulative.T[:, None, :]
    decay_mat = jnp.exp(jnp.where(causal[None], log_gaps, -jnp.inf))
    inner_prod = jnp.einsum("tgn,sgn->gts", c_groups, b_groups, preferred_element_type=f32)
    mix_weights = (jnp.repeat(inner_prod, per_group, axis=0) * decay_mat).astype(bf16)
    state_groups = entry_state.reshape(group_count, per_group, HEAD_DIM, STATE)
    y_inner = jnp.einsum("hts,shp->thp", mix_weights, scan_heads, preferred_element_type=f32)
    y_carry = jnp.einsum("tgn,grpn->tgrp", c_float, state_groups).reshape(
        tokens_here, head_count, HEAD_DIM
    )
    scan_out = y_inner + y_carry * growth[:, :, None]
    gate_float = gate_in.astype(f32)
    gate_sig = jax.nn.sigmoid(gate_float)
    gate_silu = gate_float * gate_sig
    gated = scan_out.reshape(tokens_here, -1) * gate_silu
    grouped = gated.reshape(tokens_here, group_count, -1)
    inv_rms = lax.rsqrt(jnp.mean(grouped * grouped, axis=-1, keepdims=True) + rms_epsilon)
    unit = grouped * inv_rms
    gain_groups = norm_gain.astype(f32).reshape(group_count, -1)
    mixed = (unit * gain_groups).reshape(tokens_here, -1).astype(bf16)
    mixed_line = lax.all_gather(mixed, SP[0], axis=0, tiled=True)

    columns_line = lax.all_to_all(grad_hidden, SP[0], 1, 0, tiled=True)
    outer = lax.dot_general(
        columns_line, mixed_line, (((0,), (0,)), ((), ())), preferred_element_type=f32
    )
    outer = lax.psum_scatter(outer, SP[1], scatter_dimension=0, tiled=True)
    grad_out_proj = lax.psum_scatter(outer, SP[2], scatter_dimension=0, tiled=True)

    grad_mixed = jnp.einsum("td,id->ti", grad_hidden, w_out, preferred_element_type=f32)
    grad_unit = grad_mixed.reshape(tokens_here, group_count, -1) * gain_groups
    grad_grouped = inv_rms * (grad_unit - unit * jnp.mean(grad_unit * unit, axis=-1, keepdims=True))
    grad_gated = grad_grouped.reshape(tokens_here, -1)
    grad_gate_in = (
        grad_gated
        * scan_out.reshape(tokens_here, -1)
        * gate_sig
        * (1.0 + gate_float * (1.0 - gate_sig))
    ).astype(bf16)
    grad_y = (grad_gated * gate_silu).reshape(tokens_here, head_count, HEAD_DIM)
    grad_y_b = grad_y.astype(bf16)
    grown_grads = (grad_y * growth[:, :, None]).reshape(
        tokens_here, group_count, per_group, HEAD_DIM
    )
    block_state = jnp.einsum("tgrp,tgn->grpn", grown_grads, c_float).reshape(
        expert_count, -1, STATE
    )
    rows = block_state.shape[1]
    each = expert_count // head_count
    last = jnp.repeat(cumulative[-1], each)
    sent = jnp.concatenate(
        [block_state, jnp.broadcast_to(last[:, None, None], (expert_count, 8, STATE))], axis=1
    )
    came_state = lax.all_to_all(sent, SP, 0, 0, tiled=True)
    states, lasts = came_state[:, :rows], came_state[:, rows, 0]
    through = jnp.cumsum(lasts)
    upto = jnp.concatenate([jnp.zeros((1,), f32), through[:-1]])
    blocks = jnp.arange(expert_count)
    gaps = upto[None, :] - through[:, None]
    carry = jnp.exp(jnp.where(blocks[None, :] > blocks[:, None], gaps, -jnp.inf))
    later_all = jnp.dot(
        carry, states.reshape(expert_count, -1), precision=lax.Precision.HIGHEST
    ).reshape(expert_count, rows, STATE)
    later_state = lax.all_to_all(later_all, SP, 0, 0, tiled=True)

    grad_x_inner = jnp.einsum("hts,thp->shp", mix_weights, grad_y_b, preferred_element_type=f32)
    grad_weights = (
        jnp.einsum("thp,shp->hts", grad_y_b, scan_heads, preferred_element_type=f32) * decay_mat
    )
    grad_weights = (
        grad_weights.reshape(group_count, per_group, tokens_here, tokens_here)
        .sum(axis=1)
        .astype(bf16)
    )
    grad_c_inner = jnp.einsum("gts,sgn->tgn", grad_weights, b_groups, preferred_element_type=f32)
    grad_b_inner = jnp.einsum("gts,tgn->sgn", grad_weights, c_groups, preferred_element_type=f32)
    grad_c_carry = jnp.einsum("tgrp,grpn->tgn", grown_grads, state_groups)
    x_tail = (x_float * tail_decay[:, :, None]).reshape(
        tokens_here, group_count, per_group, HEAD_DIM
    )
    later_groups = later_state.reshape(group_count, per_group, HEAD_DIM, STATE)
    grad_x_carry = jnp.einsum("sgn,grpn->sgrp", b_float, later_groups).reshape(
        tokens_here, head_count, HEAD_DIM
    )
    grad_x = grad_x_inner + grad_x_carry * tail_decay[:, :, None]
    grad_b_carry = jnp.einsum("sgrp,grpn->sgn", x_tail, later_groups)
    grad_a = jnp.sum(grad_y * scan_out, axis=2) - jnp.sum(x_float * grad_x, axis=2)
    suffix = jnp.flip(jnp.cumsum(jnp.flip(grad_a, 0), axis=0), 0)
    totals = lax.all_gather(suffix[0], SP)
    later_grad = jnp.sum(jnp.where(blocks[:, None] > sp, totals, 0.0), axis=0)
    grad_log_decay = suffix + later_grad[None, :]
    grad_scan_in = grad_x.reshape(tokens_here, -1).astype(bf16)
    grad_b_proj = (grad_b_inner + grad_b_carry).reshape(tokens_here, -1).astype(bf16)
    grad_c_proj = (grad_c_inner + grad_c_carry).reshape(tokens_here, -1).astype(bf16)
    return (
        gate_wgrad[None],
        up_wgrad[None],
        down_wgrad[None],
        grad_out_proj,
        grad_scan_in,
        grad_gate_in,
        grad_b_proj,
        grad_c_proj,
        grad_log_decay,
    )


def solution(mesh):
    split = Mesh(mesh.devices.reshape(4, 4, 4, mesh.shape["tp"]), ("sp_0", "sp_1", "sp_2", "tp"))
    return jax.shard_map(
        body,
        mesh=split,
        in_specs=(
            P(SP, None),
            P(SP, None),
            P(SP, None),
            P(SP, None),
            P(SP, None, "tp"),
            P(SP, None, "tp"),
            P(SP, None, "tp"),
            P(SP, None, "tp"),
            P(SP, "tp", None),
            P("tp", None),
            P("tp"),
            P(SP, "tp"),
            P(SP, "tp"),
            P(SP, "tp"),
            P(SP, "tp"),
            P(SP, "tp"),
            P(SP, "tp", None, None),
        ),
        out_specs=(
            P(SP, None, "tp"),
            P(SP, None, "tp"),
            P(SP, "tp", None),
            P(SP, "tp"),
            P(SP, "tp"),
            P(SP, "tp"),
            P(SP, "tp"),
            P(SP, "tp"),
            P(SP, "tp"),
        ),
        check_vma=False,
    )
```

```python
import jax
import jax.numpy as jnp
from jax import lax
from jax.experimental import pallas as pl
from jax.experimental.pallas import tpu as pltpu
from jax.sharding import Mesh
from jax.sharding import PartitionSpec as P

HEAD_DIM = 64
STATE = 128
SP = ("sp_0", "sp_1", "sp_2")


rms_epsilon = 1e-05
clamp_limit = 7.0
swish_alpha = 1.702


f32, bf16 = jnp.float32, jnp.bfloat16
MESH_ID = pl.DeviceIdType.MESH
NT = (((1,), (1,)), ((), ()))
NN = (((1,), (0,)), ((), ()))
TN = (((0,), (0,)), ((), ()))


def dotf(a, b, dims=NN):
    return lax.dot_general(a, b, dims, preferred_element_type=f32)


def place():
    z, y, x = (lax.axis_index(a) for a in SP)
    return z, y, x, z * 16 + y * 4 + x


def peer_of(k):
    z, y, x, _ = place()
    pz = lax.rem(z + k // 16, 4)
    py = lax.rem(y + lax.rem(k // 4, 4), 4)
    px = lax.rem(x + lax.rem(k, 4), 4)
    return {SP[0]: pz, SP[1]: py, SP[2]: px}, pz * 16 + py * 4 + px


def greet(others):
    barrier = pltpu.get_barrier_semaphore()

    def one(k, _):
        device, _i = peer_of(k)
        pl.semaphore_signal(barrier, inc=1, device_id=device, device_id_type=MESH_ID)
        return 0

    lax.fori_loop(1, others, one, 0)
    partner = {"tp": 1 - lax.axis_index("tp")}
    pl.semaphore_signal(barrier, inc=1, device_id=partner, device_id_type=MESH_ID)


def greeted(others):
    pl.semaphore_wait(pltpu.get_barrier_semaphore(), others)


def push(src, dst, send, recv, device):
    pltpu.make_async_remote_copy(
        src_ref=src, dst_ref=dst, send_sem=send, recv_sem=recv,
        device_id=device, device_id_type=MESH_ID,
    ).start()


def took(ref, sem):
    pltpu.make_async_copy(ref, ref, sem).wait()


def moe_kernel(
    mixer, cot, choice, weight, gate, up, wg_h, wu_h, wd_h,
    gwg_o, gwu_o, gwd_o, gh_o,
    wg, wu, wd, send_g, send_h, recv_g, recv_h, oth_g, oth_h, grads, hidden,
    fu, fg, act, acc, gg, ug, psend, precv, pown, rsend, rrecv, hot, gwg, gwu, gwd,
    wsem, lsem, sg, rg, sh, rh, dsg, drg, dsh, drh, dsp, drp, sr, rr, lr, dso, drout, osem,
):
    n = recv_g.shape[0]
    cap = recv_g.shape[1]
    half = recv_g.shape[2]
    tokens = mixer.shape[0]
    z, y, x, me = place()
    tp = lax.axis_index("tp")
    partner = {"tp": 1 - tp}
    mine = pl.ds(pl.multiple_of(tp * half, half), half)
    theirs = pl.ds(pl.multiple_of((1 - tp) * half, half), half)
    greet(n)
    loads = [
        pltpu.make_async_copy(a, b, wsem.at[i])
        for i, (a, b) in enumerate(((wd_h, wd), (wg_h, wg), (wu_h, wu)))
    ]
    for c in loads:
        c.start()
    experts = lax.broadcasted_iota(jnp.int32, (n, tokens), 0)
    hits = [experts == choice[k : k + 1, :] for k in range(2)]
    named = jnp.where(hits[0] | hits[1], 1.0, 0.0).astype(bf16)
    before = jnp.where(
        lax.broadcasted_iota(jnp.int32, (tokens, tokens), 0)
        < lax.broadcasted_iota(jnp.int32, (tokens, tokens), 1),
        1.0, 0.0,
    ).astype(bf16)
    earlier = dotf(named, before)
    places = lax.broadcasted_iota(jnp.int32, (n * cap, tokens), 0)
    hots = []
    for k in range(2):
        rank = jnp.sum(jnp.where(hits[k], earlier, 0.0), axis=0, keepdims=True)
        slot = choice[k : k + 1, :] * cap + rank.astype(jnp.int32)
        hots.append(jnp.where(places == slot, 1.0, 0.0).astype(bf16))
    hot[...] = hots[0] + hots[1]
    cot_half = cot[:, mine].astype(f32)
    rows0 = (weight[:, 0:1] * cot_half).astype(bf16)
    rows1 = (weight[:, 1:2] * cot_half).astype(bf16)
    packed = dotf(hots[0], rows0) + dotf(hots[1], rows1)
    send_g[...] = packed.reshape(n, cap, half).astype(bf16)
    packed = dotf(hot[...], mixer[:, mine])
    send_h[...] = packed.reshape(n, cap, half).astype(bf16)
    greeted(n)

    own = []
    for src, dst, sem in ((send_g, recv_g, rg), (send_h, recv_h, rh)):
        own.append(pltpu.make_async_copy(src.at[me], dst.at[me], sem.at[z]))

    def sends(src, dst, send, recv):
        def one(k, _):
            device, i = peer_of(k)
            push(src.at[i], dst.at[me], send, recv.at[z], device)
            return 0

        lax.fori_loop(1, n, one, 0)

    own[0].start()
    sends(send_g, recv_g, sg, rg)
    own[1].start()
    sends(send_h, recv_h, sh, rh)

    def prepare(i, _):
        rows = pl.ds(pl.multiple_of(i * 64, 64), 64)
        gate_full = gate[rows, :].astype(f32)
        up_full = up[rows, :].astype(f32)
        gate_clip = jnp.minimum(gate_full, clamp_limit)
        up_clip = jnp.clip(up_full, -clamp_limit, clamp_limit)
        sig = jax.nn.sigmoid(swish_alpha * gate_clip)
        swish = gate_clip * sig
        act[rows, :] = ((up_clip + 1.0) * swish).astype(bf16)
        inside = (up_full > -clamp_limit) & (up_full < clamp_limit)
        fu[rows, :] = jnp.where(inside, swish, 0.0)
        slope = sig + swish_alpha * gate_clip * sig * (1.0 - sig)
        fg[rows, :] = jnp.where(gate_full < clamp_limit, (up_clip + 1.0) * slope, 0.0)
        return 0

    lax.fori_loop(0, gate.shape[0] // 64, prepare, 0)
    for c in loads:
        c.wait()

    per = n // 4
    rowsof = per * cap

    def plane(i):
        q = lax.rem(z - i + 4, 4)
        blocks = pl.ds(pl.multiple_of(q * per, per), per)
        return q, blocks, pl.ds(pl.multiple_of(q * rowsof, rowsof), rowsof)

    def flat(ref, blocks):
        return ref[blocks].astype(f32).reshape(rowsof, half).astype(bf16)

    def arrive(i, _):
        q, blocks, rows = plane(i)
        took(recv_g.at[blocks], rg.at[q])
        push(recv_g.at[blocks], oth_g.at[blocks], dsg, drg.at[q], partner)
        g = flat(recv_g, blocks)
        grads[rows, mine] = g
        acc[rows, :] = dotf(g, wd[:, mine], NT)
        return 0

    lax.fori_loop(0, 4, arrive, 0)

    def expert(i, _):
        q, blocks, rows = plane(i)
        took(oth_g.at[blocks], drg.at[q])
        g = flat(oth_g, blocks)
        grads[rows, theirs] = g
        act_grad = acc[rows, :] + dotf(g, wd[:, theirs], NT)
        up_grad = (act_grad * fu[rows, :]).astype(bf16)
        gate_grad = (act_grad * fg[rows, :]).astype(bf16)
        ug[rows, :] = up_grad
        gg[rows, :] = gate_grad
        part = dotf(gate_grad, wg[theirs, :], NT) + dotf(up_grad, wu[theirs, :], NT)
        psend[rows, :] = part.astype(bf16)
        push(psend.at[rows], precv.at[rows], dsp, drp.at[q], partner)
        part = dotf(gate_grad, wg[mine, :], NT) + dotf(up_grad, wu[mine, :], NT)
        pown[rows, :] = part.astype(bf16)
        return 0

    lax.fori_loop(0, 4, expert, 0)

    def give_back(i, _):
        q, blocks, rows = plane(i)
        took(precv.at[rows], drp.at[q])
        total = pown[rows, :].astype(f32) + precv[rows, :].astype(f32)
        rsend[blocks] = total.reshape(per, cap, half).astype(bf16)

        def one(k, _):
            device, j = peer_of(lax.rem(4 - i, 4) * per + k)
            push(rsend.at[j], rrecv.at[me], sr, rr, device)
            return 0

        lax.fori_loop(jnp.where(i == 0, 1, 0), per, one, 0)
        return 0

    lax.fori_loop(0, 4, give_back, 0)
    back = pltpu.make_async_copy(rsend.at[me], rrecv.at[me], rr)
    back.start()

    def down(i, _):
        cols = pl.ds(pl.multiple_of(i * 512, 512), 512)
        gwd[:, cols] = dotf(act[...], grads[:, cols], TN).astype(bf16)
        pltpu.make_async_copy(gwd.at[:, cols], gwd_o.at[:, cols], osem.at[0]).start()
        return 0

    lax.fori_loop(0, grads.shape[1] // 512, down, 0)

    def arrive_h(i, _):
        q, blocks, rows = plane(i)
        took(recv_h.at[blocks], rh.at[q])
        push(recv_h.at[blocks], oth_h.at[blocks], dsh, drh.at[q], partner)
        hidden[rows, mine] = flat(recv_h, blocks)
        return 0

    lax.fori_loop(0, 4, arrive_h, 0)

    def other_h(i, _):
        q, blocks, rows = plane(i)
        took(oth_h.at[blocks], drh.at[q])
        hidden[rows, theirs] = flat(oth_h, blocks)
        return 0

    lax.fori_loop(0, 4, other_h, 0)

    def wide(i, _):
        cols = pl.ds(pl.multiple_of(i * 512, 512), 512)
        h = hidden[:, cols]
        gwg[cols, :] = dotf(h, gg[...], TN).astype(bf16)
        pltpu.make_async_copy(gwg.at[cols], gwg_o.at[cols], osem.at[1]).start()
        gwu[cols, :] = dotf(h, ug[...], TN).astype(bf16)
        pltpu.make_async_copy(gwu.at[cols], gwu_o.at[cols], osem.at[2]).start()
        return 0

    lax.fori_loop(0, hidden.shape[1] // 512, wide, 0)

    took(rrecv, rr)
    r = rrecv[...].astype(f32).reshape(n * cap, half).astype(bf16)
    moe = dotf(hot[...], r, TN)
    gh_o[:, mine] = (cot[:, mine].astype(f32) + moe).astype(bf16)
    push(gh_o.at[:, mine], gh_o.at[:, mine], dso, drout, partner)
    took(gh_o.at[:, theirs], drout)
    took(gh_o.at[:, mine], dso)
    most = pl.ds(0, n - 1)
    took(send_g.at[most], sg)
    took(send_h.at[most], sh)
    took(rsend.at[most], sr)
    took(recv_g, dsg)
    took(recv_h, dsh)
    took(psend, dsp)
    took(gwd, osem.at[0])
    took(gwg, osem.at[1])
    took(gwu, osem.at[2])


def moe_side(mixer, cot, choice, weight, gate, up, wg, wu, wd):
    n = lax.axis_size(SP)
    tokens, width = mixer.shape
    slots, hid = gate.shape
    cap, half = slots // n, width // 2
    dma = pltpu.SemaphoreType.DMA
    vm = lambda *s: pltpu.VMEM(s, bf16)
    vf = lambda *s: pltpu.VMEM(s, f32)
    inv = pl.BlockSpec(memory_space=pltpu.VMEM)
    anyv = pl.BlockSpec(memory_space=pl.ANY)
    return pl.pallas_call(
        moe_kernel,
        out_shape=(
            jax.ShapeDtypeStruct((width, hid), bf16),
            jax.ShapeDtypeStruct((width, hid), bf16),
            jax.ShapeDtypeStruct((hid, width), bf16),
            jax.ShapeDtypeStruct((tokens, width), bf16),
        ),
        in_specs=[inv] * 6 + [anyv] * 3,
        out_specs=(anyv, anyv, anyv, inv),
        scratch_shapes=[
            vm(width, hid), vm(width, hid), vm(hid, width),
            vm(n, cap, half), vm(n, cap, half), vm(n, cap, half), vm(n, cap, half),
            vm(n, cap, half), vm(n, cap, half), vm(slots, width), vm(slots, width),
            vf(slots, hid), vf(slots, hid), vm(slots, hid), vf(slots, hid),
            vm(slots, hid), vm(slots, hid), vm(slots, half), vm(slots, half), vm(slots, half),
            vm(n, cap, half), vm(n, cap, half), vm(slots, tokens),
            vm(width, hid), vm(width, hid), vm(hid, width),
            dma((3,)), dma, dma, dma((4,)), dma, dma((4,)), dma, dma((4,)), dma, dma((4,)),
            dma, dma((4,)), dma, dma, dma, dma, dma, dma((3,)),
        ],
        compiler_params=pltpu.CompilerParams(
            collective_id=1, has_side_effects=True, vmem_limit_bytes=60 * 1024 * 1024
        ),
        name="experts",
    )(mixer, cot, choice.T, weight, gate, up, wg, wu, wd)


def body(
    mixer_output,
    layer_cotangent,
    expert_choice,
    route_weight,
    gate_pre,
    up_pre,
    w_gate,
    w_up,
    w_down,
    w_out,
    norm_gain,
    scan_in,
    gate_in,
    b_proj,
    c_proj,
    log_decay,
    entry_state,
):
    f32, bf16 = jnp.float32, jnp.bfloat16
    expert_count = lax.axis_size(SP)
    sp = lax.axis_index(SP)
    tokens_here, model_width = mixer_output.shape
    gate_wgrad, up_wgrad, down_wgrad, grad_hidden = moe_side(
        mixer_output, layer_cotangent, expert_choice, route_weight,
        gate_pre[0], up_pre[0], w_gate[0], w_up[0], w_down[0],
    )

    head_count = log_decay.shape[1]
    group_count = b_proj.shape[1] // STATE
    per_group = head_count // group_count
    scan_heads = scan_in.reshape(tokens_here, head_count, HEAD_DIM)
    b_groups = b_proj.reshape(tokens_here, group_count, STATE)
    c_groups = c_proj.reshape(tokens_here, group_count, STATE)
    x_float = scan_heads.astype(f32)
    b_float = b_groups.astype(f32)
    c_float = c_groups.astype(f32)
    cumulative = jnp.cumsum(log_decay, axis=0)
    growth = jnp.exp(cumulative)
    tail_decay = jnp.exp(cumulative[-1][None, :] - cumulative)
    token_locations = jnp.arange(tokens_here)
    causal = token_locations[:, None] >= token_locations[None, :]
    log_gaps = cumulative.T[:, :, None] - cumulative.T[:, None, :]
    decay_mat = jnp.exp(jnp.where(causal[None], log_gaps, -jnp.inf))
    inner_prod = jnp.einsum("tgn,sgn->gts", c_groups, b_groups, preferred_element_type=f32)
    mix_weights = (jnp.repeat(inner_prod, per_group, axis=0) * decay_mat).astype(bf16)
    state_groups = entry_state.reshape(group_count, per_group, HEAD_DIM, STATE)
    y_inner = jnp.einsum("hts,shp->thp", mix_weights, scan_heads, preferred_element_type=f32)
    y_carry = jnp.einsum("tgn,grpn->tgrp", c_float, state_groups).reshape(
        tokens_here, head_count, HEAD_DIM
    )
    scan_out = y_inner + y_carry * growth[:, :, None]
    gate_float = gate_in.astype(f32)
    gate_sig = jax.nn.sigmoid(gate_float)
    gate_silu = gate_float * gate_sig
    gated = scan_out.reshape(tokens_here, -1) * gate_silu
    grouped = gated.reshape(tokens_here, group_count, -1)
    inv_rms = lax.rsqrt(jnp.mean(grouped * grouped, axis=-1, keepdims=True) + rms_epsilon)
    unit = grouped * inv_rms
    gain_groups = norm_gain.astype(f32).reshape(group_count, -1)
    mixed = (unit * gain_groups).reshape(tokens_here, -1).astype(bf16)
    mixed_line = lax.all_gather(mixed, SP[0], axis=0, tiled=True)

    columns_line = lax.all_to_all(grad_hidden, SP[0], 1, 0, tiled=True)
    outer = lax.dot_general(
        columns_line, mixed_line, (((0,), (0,)), ((), ())), preferred_element_type=f32
    )
    outer = lax.psum_scatter(outer, SP[1], scatter_dimension=0, tiled=True)
    grad_out_proj = lax.psum_scatter(outer, SP[2], scatter_dimension=0, tiled=True)

    grad_mixed = jnp.einsum("td,id->ti", grad_hidden, w_out, preferred_element_type=f32)
    grad_unit = grad_mixed.reshape(tokens_here, group_count, -1) * gain_groups
    grad_grouped = inv_rms * (grad_unit - unit * jnp.mean(grad_unit * unit, axis=-1, keepdims=True))
    grad_gated = grad_grouped.reshape(tokens_here, -1)
    grad_gate_in = (
        grad_gated
        * scan_out.reshape(tokens_here, -1)
        * gate_sig
        * (1.0 + gate_float * (1.0 - gate_sig))
    ).astype(bf16)
    grad_y = (grad_gated * gate_silu).reshape(tokens_here, head_count, HEAD_DIM)
    grad_y_b = grad_y.astype(bf16)
    grown_grads = (grad_y * growth[:, :, None]).reshape(
        tokens_here, group_count, per_group, HEAD_DIM
    )
    block_state = jnp.einsum("tgrp,tgn->grpn", grown_grads, c_float).reshape(
        expert_count, -1, STATE
    )
    rows = block_state.shape[1]
    each = expert_count // head_count
    last = jnp.repeat(cumulative[-1], each)
    sent = jnp.concatenate(
        [block_state, jnp.broadcast_to(last[:, None, None], (expert_count, 8, STATE))], axis=1
    )
    came_state = lax.all_to_all(sent, SP, 0, 0, tiled=True)
    states, lasts = came_state[:, :rows], came_state[:, rows, 0]
    through = jnp.cumsum(lasts)
    upto = jnp.concatenate([jnp.zeros((1,), f32), through[:-1]])
    blocks = jnp.arange(expert_count)
    gaps = upto[None, :] - through[:, None]
    carry = jnp.exp(jnp.where(blocks[None, :] > blocks[:, None], gaps, -jnp.inf))
    later_all = jnp.dot(
        carry, states.reshape(expert_count, -1), precision=lax.Precision.HIGHEST
    ).reshape(expert_count, rows, STATE)
    later_state = lax.all_to_all(later_all, SP, 0, 0, tiled=True)

    grad_x_inner = jnp.einsum("hts,thp->shp", mix_weights, grad_y_b, preferred_element_type=f32)
    grad_weights = (
        jnp.einsum("thp,shp->hts", grad_y_b, scan_heads, preferred_element_type=f32) * decay_mat
    )
    grad_weights = (
        grad_weights.reshape(group_count, per_group, tokens_here, tokens_here)
        .sum(axis=1)
        .astype(bf16)
    )
    grad_c_inner = jnp.einsum("gts,sgn->tgn", grad_weights, b_groups, preferred_element_type=f32)
    grad_b_inner = jnp.einsum("gts,tgn->sgn", grad_weights, c_groups, preferred_element_type=f32)
    grad_c_carry = jnp.einsum("tgrp,grpn->tgn", grown_grads, state_groups)
    x_tail = (x_float * tail_decay[:, :, None]).reshape(
        tokens_here, group_count, per_group, HEAD_DIM
    )
    later_groups = later_state.reshape(group_count, per_group, HEAD_DIM, STATE)
    grad_x_carry = jnp.einsum("sgn,grpn->sgrp", b_float, later_groups).reshape(
        tokens_here, head_count, HEAD_DIM
    )
    grad_x = grad_x_inner + grad_x_carry * tail_decay[:, :, None]
    grad_b_carry = jnp.einsum("sgrp,grpn->sgn", x_tail, later_groups)
    grad_a = jnp.sum(grad_y * scan_out, axis=2) - jnp.sum(x_float * grad_x, axis=2)
    suffix = jnp.flip(jnp.cumsum(jnp.flip(grad_a, 0), axis=0), 0)
    totals = suffix[0]
    for axis in reversed(SP):
        totals = lax.all_gather(totals, axis)
    totals = totals.reshape(expert_count, head_count)
    later_grad = jnp.sum(jnp.where(blocks[:, None] > sp, totals, 0.0), axis=0)
    grad_log_decay = suffix + later_grad[None, :]
    grad_scan_in = grad_x.reshape(tokens_here, -1).astype(bf16)
    grad_b_proj = (grad_b_inner + grad_b_carry).reshape(tokens_here, -1).astype(bf16)
    grad_c_proj = (grad_c_inner + grad_c_carry).reshape(tokens_here, -1).astype(bf16)
    return (
        gate_wgrad[None],
        up_wgrad[None],
        down_wgrad[None],
        grad_out_proj,
        grad_scan_in,
        grad_gate_in,
        grad_b_proj,
        grad_c_proj,
        grad_log_decay,
    )


def solution(mesh):
    split = Mesh(mesh.devices.reshape(4, 4, 4, mesh.shape["tp"]), ("sp_0", "sp_1", "sp_2", "tp"))
    return jax.shard_map(
        body,
        mesh=split,
        in_specs=(
            P(SP, None),
            P(SP, None),
            P(SP, None),
            P(SP, None),
            P(SP, None, "tp"),
            P(SP, None, "tp"),
            P(SP, None, "tp"),
            P(SP, None, "tp"),
            P(SP, "tp", None),
            P("tp", None),
            P("tp"),
            P(SP, "tp"),
            P(SP, "tp"),
            P(SP, "tp"),
            P(SP, "tp"),
            P(SP, "tp"),
            P(SP, "tp", None, None),
        ),
        out_specs=(
            P(SP, None, "tp"),
            P(SP, None, "tp"),
            P(SP, "tp", None),
            P(SP, "tp"),
            P(SP, "tp"),
            P(SP, "tp"),
            P(SP, "tp"),
            P(SP, "tp"),
            P(SP, "tp"),
        ),
        check_vma=False,
    )
```

```python
import jax
import jax.numpy as jnp
from jax import lax
from jax.experimental import pallas as pl
from jax.experimental.pallas import tpu as pltpu
from jax.sharding import Mesh
from jax.sharding import PartitionSpec as P

HEAD_DIM = 64
STATE = 128
SP = ("sp_0", "sp_1", "sp_2")


rms_epsilon = 1e-05
clamp_limit = 7.0
swish_alpha = 1.702


f32, bf16 = jnp.float32, jnp.bfloat16
MESH_ID = pl.DeviceIdType.MESH
NT = (((1,), (1,)), ((), ()))
NN = (((1,), (0,)), ((), ()))
TN = (((0,), (0,)), ((), ()))


def dotf(a, b, dims=NN):
    return lax.dot_general(a, b, dims, preferred_element_type=f32)


def place():
    z, y, x = (lax.axis_index(a) for a in SP)
    return z, y, x, z * 16 + y * 4 + x


def peer_of(k):
    z, y, x, _ = place()
    pz = lax.rem(z + k // 16, 4)
    py = lax.rem(y + lax.rem(k // 4, 4), 4)
    px = lax.rem(x + lax.rem(k, 4), 4)
    return {SP[0]: pz, SP[1]: py, SP[2]: px}, pz * 16 + py * 4 + px


def greet(others):
    barrier = pltpu.get_barrier_semaphore()

    def one(k, _):
        device, _i = peer_of(k)
        pl.semaphore_signal(barrier, inc=1, device_id=device, device_id_type=MESH_ID)
        return 0

    lax.fori_loop(1, others, one, 0)
    partner = {"tp": 1 - lax.axis_index("tp")}
    pl.semaphore_signal(barrier, inc=1, device_id=partner, device_id_type=MESH_ID)


def greeted(others):
    pl.semaphore_wait(pltpu.get_barrier_semaphore(), others)


def push(src, dst, send, recv, device):
    pltpu.make_async_remote_copy(
        src_ref=src, dst_ref=dst, send_sem=send, recv_sem=recv,
        device_id=device, device_id_type=MESH_ID,
    ).start()


def took(ref, sem):
    pltpu.make_async_copy(ref, ref, sem).wait()


def moe_kernel(
    mixer, cot, choice, weight, gate, up, wg_h, wu_h, wd_h,
    gwg_o, gwu_o, gwd_o, gh_o,
    wg, wu, wd, send_g, send_h, recv_g, recv_h, oth_g, oth_h, grads, hidden,
    fu, fg, act, acc, gg, ug, psend, precv, pown, rsend, rrecv, hot, gwg, gwu, gwd,
    wsem, lsem, sg, rg, sh, rh, dsg, drg, dsh, drh, dsp, drp, sr, rr, lr, dso, drout, osem,
):
    n = recv_g.shape[0]
    cap = recv_g.shape[1]
    half = recv_g.shape[2]
    tokens = mixer.shape[0]
    z, y, x, me = place()
    tp = lax.axis_index("tp")
    partner = {"tp": 1 - tp}
    mine = pl.ds(pl.multiple_of(tp * half, half), half)
    theirs = pl.ds(pl.multiple_of((1 - tp) * half, half), half)
    greet(n)
    loads = [
        pltpu.make_async_copy(a, b, wsem.at[i])
        for i, (a, b) in enumerate(((wd_h, wd), (wg_h, wg), (wu_h, wu)))
    ]
    for c in loads:
        c.start()
    experts = lax.broadcasted_iota(jnp.int32, (n, tokens), 0)
    hits = [experts == choice[k : k + 1, :] for k in range(2)]
    named = jnp.where(hits[0] | hits[1], 1.0, 0.0).astype(bf16)
    before = jnp.where(
        lax.broadcasted_iota(jnp.int32, (tokens, tokens), 0)
        < lax.broadcasted_iota(jnp.int32, (tokens, tokens), 1),
        1.0, 0.0,
    ).astype(bf16)
    earlier = dotf(named, before)
    places = lax.broadcasted_iota(jnp.int32, (n * cap, tokens), 0)
    hots = []
    for k in range(2):
        rank = jnp.sum(jnp.where(hits[k], earlier, 0.0), axis=0, keepdims=True)
        slot = choice[k : k + 1, :] * cap + rank.astype(jnp.int32)
        hots.append(jnp.where(places == slot, 1.0, 0.0).astype(bf16))
    hot[...] = hots[0] + hots[1]
    cot_half = cot[:, mine].astype(f32)
    rows0 = (weight[:, 0:1] * cot_half).astype(bf16)
    rows1 = (weight[:, 1:2] * cot_half).astype(bf16)
    packed = dotf(hots[0], rows0) + dotf(hots[1], rows1)
    send_g[...] = packed.reshape(n, cap, half).astype(bf16)
    packed = dotf(hot[...], mixer[:, mine])
    send_h[...] = packed.reshape(n, cap, half).astype(bf16)
    greeted(n)

    own = []
    for src, dst, sem in ((send_g, recv_g, rg), (send_h, recv_h, rh)):
        own.append(pltpu.make_async_copy(src.at[me], dst.at[me], sem.at[z]))

    def sends(src, dst, send, recv):
        def one(k, _):
            device, i = peer_of(k)
            push(src.at[i], dst.at[me], send, recv.at[z], device)
            return 0

        lax.fori_loop(1, n, one, 0)

    own[0].start()
    sends(send_g, recv_g, sg, rg)
    own[1].start()
    sends(send_h, recv_h, sh, rh)

    def prepare(i, _):
        rows = pl.ds(pl.multiple_of(i * 64, 64), 64)
        gate_full = gate[rows, :].astype(f32)
        up_full = up[rows, :].astype(f32)
        gate_clip = jnp.minimum(gate_full, clamp_limit)
        up_clip = jnp.clip(up_full, -clamp_limit, clamp_limit)
        sig = jax.nn.sigmoid(swish_alpha * gate_clip)
        swish = gate_clip * sig
        act[rows, :] = ((up_clip + 1.0) * swish).astype(bf16)
        inside = (up_full > -clamp_limit) & (up_full < clamp_limit)
        fu[rows, :] = jnp.where(inside, swish, 0.0)
        slope = sig + swish_alpha * gate_clip * sig * (1.0 - sig)
        fg[rows, :] = jnp.where(gate_full < clamp_limit, (up_clip + 1.0) * slope, 0.0)
        return 0

    lax.fori_loop(0, gate.shape[0] // 64, prepare, 0)
    for c in loads:
        c.wait()

    per = n // 4
    rowsof = per * cap

    def plane(i):
        q = lax.rem(z - i + 4, 4)
        blocks = pl.ds(pl.multiple_of(q * per, per), per)
        return q, blocks, pl.ds(pl.multiple_of(q * rowsof, rowsof), rowsof)

    def flat(ref, blocks):
        return ref[blocks].astype(f32).reshape(rowsof, half).astype(bf16)

    def arrive(i, _):
        q, blocks, rows = plane(i)
        took(recv_g.at[blocks], rg.at[q])
        push(recv_g.at[blocks], oth_g.at[blocks], dsg, drg.at[q], partner)
        g = flat(recv_g, blocks)
        grads[rows, mine] = g
        acc[rows, :] = dotf(g, wd[:, mine], NT)
        return 0

    lax.fori_loop(0, 4, arrive, 0)

    def expert(i, _):
        q, blocks, rows = plane(i)
        took(oth_g.at[blocks], drg.at[q])
        g = flat(oth_g, blocks)
        grads[rows, theirs] = g
        act_grad = acc[rows, :] + dotf(g, wd[:, theirs], NT)
        up_grad = (act_grad * fu[rows, :]).astype(bf16)
        gate_grad = (act_grad * fg[rows, :]).astype(bf16)
        ug[rows, :] = up_grad
        gg[rows, :] = gate_grad
        part = dotf(gate_grad, wg[theirs, :], NT) + dotf(up_grad, wu[theirs, :], NT)
        psend[rows, :] = part.astype(bf16)
        push(psend.at[rows], precv.at[rows], dsp, drp.at[q], partner)
        part = dotf(gate_grad, wg[mine, :], NT) + dotf(up_grad, wu[mine, :], NT)
        pown[rows, :] = part.astype(bf16)
        return 0

    lax.fori_loop(0, 4, expert, 0)

    def give_back(i, _):
        q, blocks, rows = plane(i)
        took(precv.at[rows], drp.at[q])
        total = pown[rows, :].astype(f32) + precv[rows, :].astype(f32)
        rsend[blocks] = total.reshape(per, cap, half).astype(bf16)

        def one(k, _):
            device, j = peer_of(lax.rem(4 - i, 4) * per + k)
            push(rsend.at[j], rrecv.at[me], sr, rr, device)
            return 0

        lax.fori_loop(jnp.where(i == 0, 1, 0), per, one, 0)
        return 0

    lax.fori_loop(0, 4, give_back, 0)
    back = pltpu.make_async_copy(rsend.at[me], rrecv.at[me], rr)
    back.start()

    def down(i, _):
        cols = pl.ds(pl.multiple_of(i * 512, 512), 512)
        gwd[:, cols] = dotf(act[...], grads[:, cols], TN).astype(bf16)
        pltpu.make_async_copy(gwd.at[:, cols], gwd_o.at[:, cols], osem.at[0]).start()
        return 0

    lax.fori_loop(0, grads.shape[1] // 512, down, 0)

    def arrive_h(i, _):
        q, blocks, rows = plane(i)
        took(recv_h.at[blocks], rh.at[q])
        push(recv_h.at[blocks], oth_h.at[blocks], dsh, drh.at[q], partner)
        hidden[rows, mine] = flat(recv_h, blocks)
        return 0

    lax.fori_loop(0, 4, arrive_h, 0)

    def other_h(i, _):
        q, blocks, rows = plane(i)
        took(oth_h.at[blocks], drh.at[q])
        hidden[rows, theirs] = flat(oth_h, blocks)
        return 0

    lax.fori_loop(0, 4, other_h, 0)

    def wide(i, _):
        cols = pl.ds(pl.multiple_of(i * 512, 512), 512)
        h = hidden[:, cols]
        gwg[cols, :] = dotf(h, gg[...], TN).astype(bf16)
        pltpu.make_async_copy(gwg.at[cols], gwg_o.at[cols], osem.at[1]).start()
        gwu[cols, :] = dotf(h, ug[...], TN).astype(bf16)
        pltpu.make_async_copy(gwu.at[cols], gwu_o.at[cols], osem.at[2]).start()
        return 0

    lax.fori_loop(0, hidden.shape[1] // 512, wide, 0)

    took(rrecv, rr)
    r = rrecv[...].astype(f32).reshape(n * cap, half).astype(bf16)
    moe = dotf(hot[...], r, TN)
    gh_o[:, mine] = (cot[:, mine].astype(f32) + moe).astype(bf16)
    push(gh_o.at[:, mine], gh_o.at[:, mine], dso, drout, partner)
    took(gh_o.at[:, theirs], drout)
    took(gh_o.at[:, mine], dso)
    most = pl.ds(0, n - 1)
    took(send_g.at[most], sg)
    took(send_h.at[most], sh)
    took(rsend.at[most], sr)
    took(recv_g, dsg)
    took(recv_h, dsh)
    took(psend, dsp)
    took(gwd, osem.at[0])
    took(gwg, osem.at[1])
    took(gwu, osem.at[2])


def moe_side(mixer, cot, choice, weight, gate, up, wg, wu, wd):
    n = lax.axis_size(SP)
    tokens, width = mixer.shape
    slots, hid = gate.shape
    cap, half = slots // n, width // 2
    dma = pltpu.SemaphoreType.DMA
    vm = lambda *s: pltpu.VMEM(s, bf16)
    vf = lambda *s: pltpu.VMEM(s, f32)
    inv = pl.BlockSpec(memory_space=pltpu.VMEM)
    anyv = pl.BlockSpec(memory_space=pl.ANY)
    return pl.pallas_call(
        moe_kernel,
        out_shape=(
            jax.ShapeDtypeStruct((width, hid), bf16),
            jax.ShapeDtypeStruct((width, hid), bf16),
            jax.ShapeDtypeStruct((hid, width), bf16),
            jax.ShapeDtypeStruct((tokens, width), bf16),
        ),
        in_specs=[inv] * 6 + [anyv] * 3,
        out_specs=(anyv, anyv, anyv, inv),
        scratch_shapes=[
            vm(width, hid), vm(width, hid), vm(hid, width),
            vm(n, cap, half), vm(n, cap, half), vm(n, cap, half), vm(n, cap, half),
            vm(n, cap, half), vm(n, cap, half), vm(slots, width), vm(slots, width),
            vf(slots, hid), vf(slots, hid), vm(slots, hid), vf(slots, hid),
            vm(slots, hid), vm(slots, hid), vm(slots, half), vm(slots, half), vm(slots, half),
            vm(n, cap, half), vm(n, cap, half), vm(slots, tokens),
            vm(width, hid), vm(width, hid), vm(hid, width),
            dma((3,)), dma, dma, dma((4,)), dma, dma((4,)), dma, dma((4,)), dma, dma((4,)),
            dma, dma((4,)), dma, dma, dma, dma, dma, dma((3,)),
        ],
        compiler_params=pltpu.CompilerParams(
            collective_id=1, has_side_effects=True, vmem_limit_bytes=60 * 1024 * 1024
        ),
        name="experts",
    )(mixer, cot, choice.T, weight, gate, up, wg, wu, wd)


HIGH = lax.Precision.HIGHEST


def exact(a, b, dims=NN):
    return lax.dot_general(a, b, dims, precision=HIGH, preferred_element_type=f32)


def scan_kernel(
    gh, wout_h, gain, xin, gate, bp, cp, logd, state,
    gop_o, gsi_o, ggi_o, gb_o, gc_o, gld_o,
    wout, mixl, coll, dsend, drecv, bsend, brecv, lsend, lrecv, osend, orecv, tsend, trecv,
    stb, so, unit, gy, gxi, gbi, dec, mw, mwt, xm, gym, grown,
    wsem, msn, mrv, csn, crv, dsn, drv, bsn, brv, lsn, lrv, osn, orv, tsn, trv,
):
    n, slab = bsend.shape[0], bsend.shape[1]
    tokens, width = xin.shape
    heads = logd.shape[1]
    groups = bp.shape[1] // STATE
    per = heads // groups
    gw_cols = width // groups
    z, y, x, me = place()
    plane = y * 4 + x
    greet(n)
    load = pltpu.make_async_copy(wout_h, wout, wsem)
    load.start()

    ti = lax.broadcasted_iota(jnp.int32, (tokens, tokens), 0)
    si = lax.broadcasted_iota(jnp.int32, (tokens, tokens), 1)
    lower = ti >= si
    upper = ti <= si
    ones_low = jnp.where(lower, 1.0, 0.0)
    ones_up = jnp.where(upper, 1.0, 0.0)
    cum = exact(ones_low, logd[...])
    cum_t = exact(logd[...], ones_up, TN)
    growth = jnp.exp(cum)
    tail = jnp.exp(cum[tokens - 1 : tokens, :] - cum)
    lane_head = lax.broadcasted_iota(jnp.int32, (tokens, gw_cols), 1) // HEAD_DIM
    masks = [lane_head == r for r in range(per)]
    for h in range(heads):
        dsend[h] = jnp.broadcast_to(growth[tokens - 1 : tokens, h : h + 1], dsend.shape[1:])

    def spread(v, g):
        w = jnp.broadcast_to(v[:, g * per : g * per + 1], (tokens, gw_cols))
        for r in range(1, per):
            w = jnp.where(masks[r], v[:, g * per + r : g * per + r + 1], w)
        return w

    def cols(g):
        return slice(g * gw_cols, (g + 1) * gw_cols)

    def states(g):
        return slice(g * STATE, (g + 1) * STATE)

    invs = []
    for g in range(groups):
        c, b = cp[:, states(g)], bp[:, states(g)]
        inner, inner_t = dotf(c, b, NT), dotf(b, c, NT)
        xg = xin[:, cols(g)]
        for r in range(per):
            h = g * per + r
            col, row = cum[:, h : h + 1], cum_t[h : h + 1, :]
            d = jnp.exp(jnp.where(lower, col - row, -1e30))
            dt = jnp.exp(jnp.where(upper, row - col, -1e30))
            span = slice(r * tokens, (r + 1) * tokens)
            dec[g, span, :] = d
            mw[:, span] = (inner * d).astype(bf16)
            mwt[g, :, span] = (inner_t * dt).astype(bf16)
            xm[span, :] = jnp.where(masks[r], xg.astype(f32), 0.0).astype(bf16)
        stb[cols(g), :] = state[cols(g), :].astype(bf16)
        carry = dotf(c, stb[cols(g), :], NT)
        out = dotf(mw[...], xm[...]) + carry * spread(growth, g)
        so[:, cols(g)] = out
        gf = gate[:, cols(g)].astype(f32)
        gated = out * (gf * jax.nn.sigmoid(gf))
        inv = lax.rsqrt(jnp.mean(gated * gated, axis=1, keepdims=True) + rms_epsilon)
        invs.append(inv)
        u = gated * inv
        unit[:, cols(g)] = u
        mixl[z, :, cols(g)] = (u * gain[:, cols(g)].astype(f32)).astype(bf16)

    quarter = gh.shape[1] // 4
    coll[z] = gh[:, pl.ds(pl.multiple_of(z * quarter, quarter), quarter)]
    greeted(n)
    for k in range(1, 4):
        pz = lax.rem(z + k, 4)
        part = pl.ds(pl.multiple_of(pz * quarter, quarter), quarter)
        push(gh.at[:, part], coll.at[z], csn, crv, {SP[0]: pz})

    def send_decay(k, _):
        device, j = peer_of(k)
        push(dsend.at[j // (n // heads)], drecv.at[me], dsn, drv, device)
        return 0

    lax.fori_loop(1, n, send_decay, 0)
    own_decay = pltpu.make_async_copy(dsend.at[me // (n // heads)], drecv.at[me], drv)
    own_decay.start()
    for k in range(1, 4):
        push(mixl.at[z], mixl.at[z], msn, mrv, {SP[0]: lax.rem(z + k, 4)})
    load.wait()

    slabs = gw_cols // slab
    for g in range(groups):
        c = cp[:, states(g)]
        gain_f = gain[:, cols(g)].astype(f32)
        gu = dotf(gh[...], wout[cols(g), :], NT) * gain_f
        u = unit[:, cols(g)]
        out = so[:, cols(g)]
        gg = invs[g] * (gu - u * jnp.mean(gu * u, axis=1, keepdims=True))
        gf = gate[:, cols(g)].astype(f32)
        sig = jax.nn.sigmoid(gf)
        ggi_o[:, cols(g)] = (gg * out * sig * (1.0 + gf * (1.0 - sig))).astype(bf16)
        gyg = gg * (gf * sig)
        gy[:, cols(g)] = gyg
        gr = (gyg * spread(growth, g)).astype(bf16)
        grown[:, cols(g)] = gr
        bs = dotf(gr, c, TN)
        bsend[g * slabs : (g + 1) * slabs] = bs.reshape(slabs, slab, STATE).astype(bf16)

    def sends(src, dst, send, recv):
        def one(k, _):
            device, j = peer_of(k)
            push(src.at[j], dst.at[me], send, recv, device)
            return 0

        lax.fori_loop(1, n, one, 0)
        pltpu.make_async_copy(src.at[me], dst.at[me], recv).start()

    sends(bsend, brecv, bsn, brv)

    for g in range(groups):
        c, b = cp[:, states(g)], bp[:, states(g)]
        xg = xin[:, cols(g)]
        gyg = gy[:, cols(g)]
        for r in range(per):
            gym[r * tokens : (r + 1) * tokens, :] = jnp.where(masks[r], gyg, 0.0).astype(bf16)
        pairs = dotf(gym[...], xg, NT) * dec[g]
        gw = pairs[:tokens]
        for r in range(1, per):
            gw = gw + pairs[r * tokens : (r + 1) * tokens]
        gw = gw.astype(bf16)
        gxi[:, cols(g)] = dotf(mwt[g], gym[...])
        gc = dotf(gw, b) + dotf(grown[:, cols(g)], stb[cols(g), :])
        gc_o[:, states(g)] = gc.astype(bf16)
        gbi[:, states(g)] = dotf(gw, c, TN)

    took(coll.at[pl.ds(0, 3)], crv)
    took(mixl.at[pl.ds(0, 3)], mrv)
    rows = osend.shape[1]
    left = coll[...].reshape(4 * tokens, quarter)
    right = mixl[...].reshape(4 * tokens, width)
    osend[...] = dotf(left, right, TN).astype(bf16).reshape(n // 4, rows, width)

    took(brecv, brv)
    took(drecv, drv)

    def step(i, acc):
        j = n - 1 - i
        lsend[j] = acc.reshape(slab, STATE).astype(bf16)
        block = brecv[j].astype(f32).reshape(slab // 8, 8, STATE)
        return acc * drecv[j][None] + block

    lax.fori_loop(0, n, step, jnp.zeros((slab // 8, 8, STATE), f32), unroll=4)
    sends(lsend, lrecv, lsn, lrv)

    def send_outer(k, _):
        py, px = lax.rem(y + k // 4, 4), lax.rem(x + lax.rem(k, 4), 4)
        push(osend.at[py * 4 + px], orecv.at[plane], osn, orv, {SP[1]: py, SP[2]: px})
        return 0

    lax.fori_loop(1, n // 4, send_outer, 0)
    pltpu.make_async_copy(osend.at[plane], orecv.at[plane], orv).start()

    took(lrecv, lrv)
    ga = jnp.zeros((tokens, STATE), f32)
    for g in range(groups):
        b = bp[:, states(g)]
        xf = xin[:, cols(g)].astype(f32)
        later = lrecv[g * slabs : (g + 1) * slabs].reshape(gw_cols, STATE)
        tails = spread(tail, g)
        gx = gxi[:, cols(g)] + dotf(b, later, NT) * tails
        gsi_o[:, cols(g)] = gx.astype(bf16)
        gb = gbi[:, states(g)] + dotf((xf * tails).astype(bf16), later)
        gb_o[:, states(g)] = gb.astype(bf16)
        sel = jnp.where(
            lax.broadcasted_iota(jnp.int32, (gw_cols, STATE), 0) // HEAD_DIM + g * per
            == lax.broadcasted_iota(jnp.int32, (gw_cols, STATE), 1),
            1.0, 0.0,
        )
        ga = ga + exact(gy[:, cols(g)] * so[:, cols(g)] - xf * gx, sel)
    suffix = exact(ones_up, ga)
    tsend[...] = jnp.broadcast_to(suffix[0:1, :], tsend.shape)

    def send_total(k, _):
        device, _j = peer_of(k)
        push(tsend, trecv.at[me], tsn, trv, device)
        return 0

    lax.fori_loop(1, n, send_total, 0)
    took(orecv, orv)
    total = orecv[0].astype(f32)
    for k in range(1, n // 4):
        total = total + orecv[k].astype(f32)
    gop_o[...] = total
    most = pl.ds(0, n - 1)
    took(trecv.at[most], trv)
    after = lax.fori_loop(
        me + 1, n, lambda j, t: t + trecv[j], jnp.zeros(tsend.shape, f32)
    )
    gld_o[...] = (suffix + after[0:1, :])[:, :heads]

    took(coll.at[pl.ds(0, 3)], csn)
    took(mixl.at[pl.ds(0, 3)], msn)
    took(drecv.at[most], dsn)
    took(bsend.at[most], bsn)
    took(lsend.at[most], lsn)
    took(osend.at[pl.ds(0, n // 4 - 1)], osn)
    took(trecv.at[most], tsn)


def mixer_side(gh, wout, gain, xin, gate, bp, cp, logd, state):
    n = lax.axis_size(SP)
    tokens, width = xin.shape
    heads = logd.shape[1]
    groups = bp.shape[1] // STATE
    per = heads // groups
    slab = heads * HEAD_DIM // n
    dwidth = gh.shape[1]
    rows = dwidth // n
    dma = pltpu.SemaphoreType.DMA
    vm = lambda *s: pltpu.VMEM(s, bf16)
    vf = lambda *s: pltpu.VMEM(s, f32)
    inv = pl.BlockSpec(memory_space=pltpu.VMEM)
    anyv = pl.BlockSpec(memory_space=pl.ANY)
    return pl.pallas_call(
        scan_kernel,
        out_shape=(
            jax.ShapeDtypeStruct((rows, width), f32),
            jax.ShapeDtypeStruct((tokens, width), bf16),
            jax.ShapeDtypeStruct((tokens, width), bf16),
            jax.ShapeDtypeStruct(bp.shape, bf16),
            jax.ShapeDtypeStruct(cp.shape, bf16),
            jax.ShapeDtypeStruct((tokens, heads), f32),
        ),
        in_specs=[inv, anyv] + [inv] * 7,
        out_specs=(inv,) * 6,
        scratch_shapes=[
            vm(*wout.shape), vm(4, tokens, width), vm(4, tokens, dwidth // 4),
            vf(heads, 8, STATE), vf(n, 8, STATE),
            vm(n, slab, STATE), vm(n, slab, STATE), vm(n, slab, STATE), vm(n, slab, STATE),
            vm(n // 4, rows, width), vm(n // 4, rows, width),
            vf(8, STATE), vf(n, 8, STATE),
            vm(width, STATE), vf(tokens, width), vf(tokens, width), vf(tokens, width),
            vf(tokens, width), vf(tokens, groups * STATE),
            vf(groups, per * tokens, tokens), vm(tokens, per * tokens),
            vm(groups, tokens, per * tokens), vm(per * tokens, width // groups),
            vm(per * tokens, width // groups), vm(tokens, width),
        ]
        + [dma] * 15,
        compiler_params=pltpu.CompilerParams(
            collective_id=2, has_side_effects=True, vmem_limit_bytes=60 * 1024 * 1024
        ),
        name="mixer",
    )(gh, wout, gain, xin, gate, bp, cp, logd, state)


def body(
    mixer_output,
    layer_cotangent,
    expert_choice,
    route_weight,
    gate_pre,
    up_pre,
    w_gate,
    w_up,
    w_down,
    w_out,
    norm_gain,
    scan_in,
    gate_in,
    b_proj,
    c_proj,
    log_decay,
    entry_state,
):
    state = entry_state.reshape(-1, STATE)
    gate_wgrad, up_wgrad, down_wgrad, grad_hidden = moe_side(
        mixer_output, layer_cotangent, expert_choice, route_weight,
        gate_pre[0], up_pre[0], w_gate[0], w_up[0], w_down[0],
    )
    rest = mixer_side(
        grad_hidden, w_out, norm_gain[None], scan_in, gate_in, b_proj, c_proj, log_decay, state
    )
    return (gate_wgrad[None], up_wgrad[None], down_wgrad[None], *rest)


def solution(mesh):
    split = Mesh(mesh.devices.reshape(4, 4, 4, mesh.shape["tp"]), ("sp_0", "sp_1", "sp_2", "tp"))
    return jax.shard_map(
        body,
        mesh=split,
        in_specs=(
            P(SP, None),
            P(SP, None),
            P(SP, None),
            P(SP, None),
            P(SP, None, "tp"),
            P(SP, None, "tp"),
            P(SP, None, "tp"),
            P(SP, None, "tp"),
            P(SP, "tp", None),
            P("tp", None),
            P("tp"),
            P(SP, "tp"),
            P(SP, "tp"),
            P(SP, "tp"),
            P(SP, "tp"),
            P(SP, "tp"),
            P(SP, "tp", None, None),
        ),
        out_specs=(
            P(SP, None, "tp"),
            P(SP, None, "tp"),
            P(SP, "tp", None),
            P(SP, "tp"),
            P(SP, "tp"),
            P(SP, "tp"),
            P(SP, "tp"),
            P(SP, "tp"),
            P(SP, "tp"),
        ),
        check_vma=False,
    )
```

```python
import jax
import jax.numpy as jnp
from jax import lax
from jax.experimental import pallas as pl
from jax.experimental.pallas import tpu as pltpu
from jax.sharding import Mesh
from jax.sharding import PartitionSpec as P

HEAD_DIM = 64
STATE = 128
SP = ("sp_0", "sp_1", "sp_2")


rms_epsilon = 1e-05
clamp_limit = 7.0
swish_alpha = 1.702


f32, bf16 = jnp.float32, jnp.bfloat16
MESH_ID = pl.DeviceIdType.MESH
NT = (((1,), (1,)), ((), ()))
NN = (((1,), (0,)), ((), ()))
TN = (((0,), (0,)), ((), ()))


def dotf(a, b, dims=NN):
    return lax.dot_general(a, b, dims, preferred_element_type=f32)


def place():
    z, y, x = (lax.axis_index(a) for a in SP)
    return z, y, x, z * 16 + y * 4 + x


def peer_of(k):
    z, y, x, _ = place()
    pz = lax.rem(z + k // 16, 4)
    py = lax.rem(y + lax.rem(k // 4, 4), 4)
    px = lax.rem(x + lax.rem(k, 4), 4)
    return {SP[0]: pz, SP[1]: py, SP[2]: px}, pz * 16 + py * 4 + px


def greet(others):
    barrier = pltpu.get_barrier_semaphore()

    def one(k, _):
        device, _i = peer_of(k)
        pl.semaphore_signal(barrier, inc=1, device_id=device, device_id_type=MESH_ID)
        return 0

    lax.fori_loop(1, others, one, 0)
    partner = {"tp": 1 - lax.axis_index("tp")}
    pl.semaphore_signal(barrier, inc=1, device_id=partner, device_id_type=MESH_ID)


def greeted(others):
    pl.semaphore_wait(pltpu.get_barrier_semaphore(), others)


def push(src, dst, send, recv, device):
    pltpu.make_async_remote_copy(
        src_ref=src, dst_ref=dst, send_sem=send, recv_sem=recv,
        device_id=device, device_id_type=MESH_ID,
    ).start()


def took(ref, sem):
    pltpu.make_async_copy(ref, ref, sem).wait()


HIGH = lax.Precision.HIGHEST
EARLY = 2
MIX = 0
REST = 3
COLL = 1


def exact(a, b, dims=NN):
    return lax.dot_general(a, b, dims, precision=HIGH, preferred_element_type=f32)


def whole_kernel(
    cot, choice, weight, logd, gain,
    mixer_h, gate_h, up_h, wd_h, wg_h, wu_h, wout_h, xin_h, gin_h, bp_h, cp_h, state_h,
    gwg, gwu, gwd, gop_o, gsi_o, ggi_o, gb_o, gc_o, gld_o,
    mixer, gate, up, wd, wg, wu, wout, xin, gin, bp, cp, state,
    send_g, send_h, recv_g, recv_h, oth_g, oth_h, grads, hidden,
    fu, fg, act, acc, gg, ug, psend, precv, pown, rsend, rrecv, hot,
    gh, mixl, coll, dsend, drecv, bsend, brecv, lsend, lrecv, osend, orecv, tsend, trecv,
    stb, so, unit, gy, gxi, gbi, dec, mw, mwt, xm, gym, grown,
    wsem, sg, rg, sh, rh, dsg, drg, dsh, drh, dsp, drp, sr, rr, dso, drout,
    msn, mrv, csn, crv, dsn, drv, bsn, brv, lsn, lrv, osn, orv, tsn, trv,
):
    n, cap, half = recv_g.shape
    tokens = cot.shape[0]
    z, y, x, me = place()
    plane_at = y * 4 + x
    tp = lax.axis_index("tp")
    partner = {"tp": 1 - tp}
    mine = pl.ds(pl.multiple_of(tp * half, half), half)
    theirs = pl.ds(pl.multiple_of((1 - tp) * half, half), half)
    most = pl.ds(0, n - 1)
    greet(n)
    order = (
        (xin_h, xin), (gin_h, gin), (bp_h, bp), (cp_h, cp), (state_h, state), (mixer_h, mixer),
        (gate_h, gate), (up_h, up), (wd_h, wd), (wg_h, wg), (wu_h, wu), (wout_h, wout),
    )
    loads = [pltpu.make_async_copy(a, b, wsem.at[i]) for i, (a, b) in enumerate(order)]
    for c in loads:
        c.start()

    ti = lax.broadcasted_iota(jnp.int32, (tokens, tokens), 0)
    si = lax.broadcasted_iota(jnp.int32, (tokens, tokens), 1)
    lower = ti >= si
    upper = ti <= si
    experts = lax.broadcasted_iota(jnp.int32, (n, tokens), 0)
    hits = [experts == choice[k : k + 1, :] for k in range(2)]
    named = jnp.where(hits[0] | hits[1], 1.0, 0.0).astype(bf16)
    before = jnp.where(ti < si, 1.0, 0.0).astype(bf16)
    earlier = dotf(named, before)
    places = lax.broadcasted_iota(jnp.int32, (n * cap, tokens), 0)
    hots = []
    for k in range(2):
        rank = jnp.sum(jnp.where(hits[k], earlier, 0.0), axis=0, keepdims=True)
        slot = choice[k : k + 1, :] * cap + rank.astype(jnp.int32)
        hots.append(jnp.where(places == slot, 1.0, 0.0).astype(bf16))
    hot[...] = hots[0] + hots[1]
    weights = exact(jnp.where(ti == si, 1.0, 0.0), weight[...], NT)
    cot_half = cot[:, mine].astype(f32)
    rows0 = (weights[:, 0:1] * cot_half).astype(bf16)
    rows1 = (weights[:, 1:2] * cot_half).astype(bf16)
    packed = dotf(hots[0], rows0) + dotf(hots[1], rows1)
    send_g[...] = packed.reshape(n, cap, half).astype(bf16)
    greeted(n)

    def sends(src, dst, send, recv, first, last):
        def one(k, _):
            device, i = peer_of(k)
            push(src.at[i], dst.at[me], send, recv, device)
            return 0

        lax.fori_loop(first, last, one, 0)

    pltpu.make_async_copy(send_g.at[me], recv_g.at[me], rg.at[z]).start()
    sends(send_g, recv_g, sg, rg.at[z], 1, n)

    heads = logd.shape[0]
    groups = bp.shape[1] // STATE
    width = xin.shape[1]
    per = heads // groups
    gw_cols = width // groups
    ones_low = jnp.where(lower, 1.0, 0.0)
    ones_up = jnp.where(upper, 1.0, 0.0)
    cum = exact(ones_low, logd[...], NT)
    cum_t = exact(logd[...], ones_up)
    growth = jnp.exp(cum)
    tail = jnp.exp(cum[tokens - 1 : tokens, :] - cum)
    lane_head = lax.broadcasted_iota(jnp.int32, (tokens, gw_cols), 1) // HEAD_DIM
    masks = [lane_head == r for r in range(per)]
    for h in range(heads):
        dsend[h] = jnp.broadcast_to(growth[tokens - 1 : tokens, h : h + 1], dsend.shape[1:])
    each = n // heads
    pltpu.make_async_copy(dsend.at[me // each], drecv.at[me], drv).start()

    def send_decay(k, _):
        device, j = peer_of(k)
        push(dsend.at[j // each], drecv.at[me], dsn, drv, device)
        return 0

    lax.fori_loop(1, n, send_decay, 0)

    def spread(v, g):
        w = jnp.broadcast_to(v[:, g * per : g * per + 1], (tokens, gw_cols))
        for r in range(1, per):
            w = jnp.where(masks[r], v[:, g * per + r : g * per + r + 1], w)
        return w

    def cols(g):
        return slice(g * gw_cols, (g + 1) * gw_cols)

    def states(g):
        return slice(g * STATE, (g + 1) * STATE)

    for c in loads[:5]:
        c.wait()
    invs = []
    for g in range(groups):
        c, b = cp[:, states(g)], bp[:, states(g)]
        inner, inner_t = dotf(c, b, NT), dotf(b, c, NT)
        xg = xin[:, cols(g)]
        for r in range(per):
            h = g * per + r
            col, row = cum[:, h : h + 1], cum_t[h : h + 1, :]
            d = jnp.exp(jnp.where(lower, col - row, -1e30))
            dt = jnp.exp(jnp.where(upper, row - col, -1e30))
            span = slice(r * tokens, (r + 1) * tokens)
            dec[g, span, :] = d
            mw[:, span] = (inner * d).astype(bf16)
            mwt[g, :, span] = (inner_t * dt).astype(bf16)
            xm[span, :] = jnp.where(masks[r], xg.astype(f32), 0.0).astype(bf16)
        stb[cols(g), :] = state[cols(g), :].astype(bf16)
        carry = dotf(c, stb[cols(g), :], NT)
        out = dotf(mw[...], xm[...]) + carry * spread(growth, g)
        so[:, cols(g)] = out
        gf = gin[:, cols(g)].astype(f32)
        gated = out * (gf * jax.nn.sigmoid(gf))
        inv = lax.rsqrt(jnp.mean(gated * gated, axis=1, keepdims=True) + rms_epsilon)
        invs.append(inv)
        u = gated * inv
        unit[:, cols(g)] = u
        mixl[z, :, cols(g)] = (u * gain[:, cols(g)].astype(f32)).astype(bf16)

    def send_mixed():
        for k in range(1, 4):
            push(mixl.at[z], mixl.at[z], msn, mrv, {SP[0]: lax.rem(z + k, 4)})

    if MIX == 0:
        send_mixed()

    loads[5].wait()
    packed = dotf(hot[...], mixer[:, mine])
    send_h[...] = packed.reshape(n, cap, half).astype(bf16)
    pltpu.make_async_copy(send_h.at[me], recv_h.at[me], rh.at[z]).start()

    loads[6].wait()
    loads[7].wait()

    def prepare(i, _):
        rows = pl.ds(pl.multiple_of(i * 64, 64), 64)
        gate_full = gate[rows, :].astype(f32)
        up_full = up[rows, :].astype(f32)
        gate_clip = jnp.minimum(gate_full, clamp_limit)
        up_clip = jnp.clip(up_full, -clamp_limit, clamp_limit)
        sig = jax.nn.sigmoid(swish_alpha * gate_clip)
        swish = gate_clip * sig
        act[rows, :] = ((up_clip + 1.0) * swish).astype(bf16)
        inside = (up_full > -clamp_limit) & (up_full < clamp_limit)
        fu[rows, :] = jnp.where(inside, swish, 0.0)
        slope = sig + swish_alpha * gate_clip * sig * (1.0 - sig)
        fg[rows, :] = jnp.where(gate_full < clamp_limit, (up_clip + 1.0) * slope, 0.0)
        return 0

    lax.fori_loop(0, gate.shape[0] // 64, prepare, 0)
    for c in loads[8:11]:
        c.wait()

    quart = n // 4
    rowsof = quart * cap

    def plane(i):
        q = lax.rem(z - i + 4, 4)
        blocks = pl.ds(pl.multiple_of(q * quart, quart), quart)
        return q, blocks, pl.ds(pl.multiple_of(q * rowsof, rowsof), rowsof)

    def flat(ref, blocks):
        return ref[blocks].astype(f32).reshape(rowsof, half).astype(bf16)

    def arrive(i, _):
        q, blocks, rows = plane(i)
        took(recv_g.at[blocks], rg.at[q])
        push(recv_g.at[blocks], oth_g.at[blocks], dsg, drg.at[q], partner)
        g = flat(recv_g, blocks)
        grads[rows, mine] = g
        acc[rows, :] = dotf(g, wd[:, mine], NT)
        return 0


    def expert(i, _):
        q, blocks, rows = plane(i)
        took(oth_g.at[blocks], drg.at[q])
        g = flat(oth_g, blocks)
        grads[rows, theirs] = g
        act_grad = acc[rows, :] + dotf(g, wd[:, theirs], NT)
        up_grad = (act_grad * fu[rows, :]).astype(bf16)
        gate_grad = (act_grad * fg[rows, :]).astype(bf16)
        ug[rows, :] = up_grad
        gg[rows, :] = gate_grad
        part = dotf(gate_grad, wg[theirs, :], NT) + dotf(up_grad, wu[theirs, :], NT)
        psend[rows, :] = part.astype(bf16)
        push(psend.at[rows], precv.at[rows], dsp, drp.at[q], partner)
        part = dotf(gate_grad, wg[mine, :], NT) + dotf(up_grad, wu[mine, :], NT)
        pown[rows, :] = part.astype(bf16)
        return 0


    def give_back(i, _):
        q, blocks, rows = plane(i)
        took(precv.at[rows], drp.at[q])
        total = pown[rows, :].astype(f32) + precv[rows, :].astype(f32)
        rsend[blocks] = total.reshape(quart, cap, half).astype(bf16)

        def one(k, _):
            device, j = peer_of((4 - i) % 4 * quart + k)
            push(rsend.at[j], rrecv.at[me], sr, rr, device)
            return 0

        lax.fori_loop(1 if i == 0 else 0, quart, one, 0)
        return 0

    arrive(0, 0)
    expert(0, 0)
    give_back(0, 0)
    arrive(1, 0)
    arrive(2, 0)
    expert(1, 0)
    arrive(3, 0)
    sends(send_h, recv_h, sh, rh.at[z], 1, max(1, EARLY * n // 4))
    expert(2, 0)
    give_back(1, 0)
    expert(3, 0)
    give_back(2, 0)
    give_back(3, 0)
    def send_rest(at):
        if REST == at:
            sends(send_h, recv_h, sh, rh.at[z], max(1, EARLY * n // 4), n)

    send_rest(0)
    pltpu.make_async_copy(rsend.at[me], rrecv.at[me], rr).start()

    def down(i, _):
        cols = pl.ds(pl.multiple_of(i * 512, 512), 512)
        gwd[:, cols] = dotf(act[...], grads[:, cols], TN).astype(bf16)
        return 0

    lax.fori_loop(0, grads.shape[1] // 512, down, 0)

    loads[11].wait()
    took(rrecv, rr)
    r = rrecv[...].astype(f32).reshape(n * cap, half).astype(bf16)
    gh[:, mine] = (cot[:, mine].astype(f32) + dotf(hot[...], r, TN)).astype(bf16)
    push(gh.at[:, mine], gh.at[:, mine], dso, drout, partner)
    took(gh.at[:, theirs], drout)
    quarter = gh.shape[1] // 4

    def send_columns():
        for k in range(1, 4):
            pz = lax.rem(z + k, 4)
            part = pl.ds(pl.multiple_of(pz * quarter, quarter), quarter)
            push(gh.at[:, part], coll.at[z], csn, crv, {SP[0]: pz})

    if COLL == 0:
        send_columns()
    coll[z] = gh[:, pl.ds(pl.multiple_of(z * quarter, quarter), quarter)]
    send_rest(1)
    slab = bsend.shape[1]
    slabs = gw_cols // slab
    for g in range(groups):
        c = cp[:, states(g)]
        gain_f = gain[:, cols(g)].astype(f32)
        gu = dotf(gh[...], wout[cols(g), :], NT) * gain_f
        u = unit[:, cols(g)]
        out = so[:, cols(g)]
        dgated = invs[g] * (gu - u * jnp.mean(gu * u, axis=1, keepdims=True))
        gf = gin[:, cols(g)].astype(f32)
        sig = jax.nn.sigmoid(gf)
        ggi_o[:, cols(g)] = (dgated * out * sig * (1.0 + gf * (1.0 - sig))).astype(bf16)
        gyg = dgated * (gf * sig)
        gy[:, cols(g)] = gyg
        gr = (gyg * spread(growth, g)).astype(bf16)
        grown[:, cols(g)] = gr
        bs = dotf(gr, c, TN)
        bsend[g * slabs : (g + 1) * slabs] = bs.reshape(slabs, slab, STATE).astype(bf16)

    def exchange(src, dst, send, recv):
        sends(src, dst, send, recv, 1, n)
        pltpu.make_async_copy(src.at[me], dst.at[me], recv).start()

    exchange(bsend, brecv, bsn, brv)
    if COLL == 1:
        send_columns()
    send_rest(2)
    if MIX == 1:
        send_mixed()

    for g in range(groups):
        c, b = cp[:, states(g)], bp[:, states(g)]
        xg = xin[:, cols(g)]
        gyg = gy[:, cols(g)]
        for r in range(per):
            gym[r * tokens : (r + 1) * tokens, :] = jnp.where(masks[r], gyg, 0.0).astype(bf16)
        pairs = dotf(gym[...], xg, NT) * dec[g]
        gw = pairs[:tokens]
        for r in range(1, per):
            gw = gw + pairs[r * tokens : (r + 1) * tokens]
        gw = gw.astype(bf16)
        gxi[:, cols(g)] = dotf(mwt[g], gym[...])
        gc = dotf(gw, b) + dotf(grown[:, cols(g)], stb[cols(g), :])
        gc_o[:, states(g)] = gc.astype(bf16)
        gbi[:, states(g)] = dotf(gw, c, TN)

    took(brecv, brv)
    took(drecv, drv)

    def step(i, acc):
        j = n - 1 - i
        lsend[j] = acc.reshape(slab, STATE).astype(bf16)
        block = brecv[j].astype(f32).reshape(slab // 8, 8, STATE)
        return acc * drecv[j][None] + block

    lax.fori_loop(0, n, step, jnp.zeros((slab // 8, 8, STATE), f32), unroll=4)
    exchange(lsend, lrecv, lsn, lrv)
    send_rest(3)

    took(coll.at[pl.ds(0, 3)], crv)
    took(mixl.at[pl.ds(0, 3)], mrv)
    rows = osend.shape[1]
    left = coll[...].reshape(4 * tokens, quarter)
    right = mixl[...].reshape(4 * tokens, width)
    osend[...] = dotf(left, right, TN).astype(bf16).reshape(n // 4, rows, width)

    def send_outer(k, _):
        py, px = lax.rem(y + k // 4, 4), lax.rem(x + lax.rem(k, 4), 4)
        push(osend.at[py * 4 + px], orecv.at[plane_at], osn, orv, {SP[1]: py, SP[2]: px})
        return 0

    lax.fori_loop(1, n // 4, send_outer, 0)
    pltpu.make_async_copy(osend.at[plane_at], orecv.at[plane_at], orv).start()

    send_rest(4)

    def arrive_h(i, _):
        q, blocks, rows = plane(i)
        took(recv_h.at[blocks], rh.at[q])
        push(recv_h.at[blocks], oth_h.at[blocks], dsh, drh.at[q], partner)
        hidden[rows, mine] = flat(recv_h, blocks)
        return 0

    lax.fori_loop(0, 4, arrive_h, 0)

    def other_h(i, _):
        q, blocks, rows = plane(i)
        took(oth_h.at[blocks], drh.at[q])
        hidden[rows, theirs] = flat(oth_h, blocks)
        return 0

    lax.fori_loop(0, 4, other_h, 0)

    def wide(i, _):
        cols = pl.ds(pl.multiple_of(i * 512, 512), 512)
        h = hidden[:, cols]
        gwg[cols, :] = dotf(h, gg[...], TN).astype(bf16)
        gwu[cols, :] = dotf(h, ug[...], TN).astype(bf16)
        return 0

    lax.fori_loop(0, hidden.shape[1] // 512, wide, 0)

    took(lrecv, lrv)
    ga = jnp.zeros((tokens, STATE), f32)
    for g in range(groups):
        b = bp[:, states(g)]
        xf = xin[:, cols(g)].astype(f32)
        later = lrecv[g * slabs : (g + 1) * slabs].reshape(gw_cols, STATE)
        tails = spread(tail, g)
        gx = gxi[:, cols(g)] + dotf(b, later, NT) * tails
        gsi_o[:, cols(g)] = gx.astype(bf16)
        gb = gbi[:, states(g)] + dotf((xf * tails).astype(bf16), later)
        gb_o[:, states(g)] = gb.astype(bf16)
        sel = jnp.where(
            lax.broadcasted_iota(jnp.int32, (gw_cols, STATE), 0) // HEAD_DIM + g * per
            == lax.broadcasted_iota(jnp.int32, (gw_cols, STATE), 1),
            1.0, 0.0,
        )
        ga = ga + exact(gy[:, cols(g)] * so[:, cols(g)] - xf * gx, sel)
    suffix = exact(ones_up, ga)
    tsend[...] = jnp.broadcast_to(suffix[0:1, :], tsend.shape)

    def send_total(k, _):
        device, _j = peer_of(k)
        push(tsend, trecv.at[me], tsn, trv, device)
        return 0

    lax.fori_loop(1, n, send_total, 0)
    took(orecv, orv)
    total = orecv[0].astype(f32)
    for k in range(1, n // 4):
        total = total + orecv[k].astype(f32)
    gop_o[...] = total
    took(trecv.at[most], trv)
    after = lax.fori_loop(
        me + 1, n, lambda j, t: t + trecv[j], jnp.zeros(tsend.shape, f32)
    )
    total = suffix + after[0:1, :]
    gld_o[...] = exact(total, jnp.where(ti == si, 1.0, 0.0), TN)[:heads, :]

    took(coll.at[pl.ds(0, 3)], csn)
    took(mixl.at[pl.ds(0, 3)], msn)
    took(drecv.at[most], dsn)
    took(bsend.at[most], bsn)
    took(lsend.at[most], lsn)
    took(osend.at[pl.ds(0, n // 4 - 1)], osn)
    took(trecv.at[most], tsn)
    took(gh.at[:, mine], dso)
    took(send_g.at[most], sg)
    took(send_h.at[most], sh)
    took(rsend.at[most], sr)
    took(recv_g, dsg)
    took(recv_h, dsh)
    took(psend, dsp)


def whole(cot, choice, weight, logd, gain, mixer, gate, up, wd, wg, wu, wout, xin, gin, bp, cp, state):
    n = lax.axis_size(SP)
    tokens, dwidth = cot.shape
    slots, hid = gate.shape
    cap, half = slots // n, dwidth // 2
    width = xin.shape[1]
    heads = logd.shape[0]
    groups = bp.shape[1] // STATE
    per = heads // groups
    slab = heads * HEAD_DIM // n
    rows = dwidth // n
    dma = pltpu.SemaphoreType.DMA
    vm = lambda *s: pltpu.VMEM(s, bf16)
    vf = lambda *s: pltpu.VMEM(s, f32)
    inv = pl.BlockSpec(memory_space=pltpu.VMEM)
    anyv = pl.BlockSpec(memory_space=pl.ANY)
    bulk = (mixer, gate, up, wd, wg, wu, wout, xin, gin, bp, cp, state)
    shaped = lambda s, t: pltpu.VMEM(s, t)
    return pl.pallas_call(
        whole_kernel,
        out_shape=(
            shaped((dwidth, hid), bf16), shaped((dwidth, hid), bf16), shaped((hid, dwidth), bf16),
            shaped((rows, width), f32),
            shaped((tokens, width), bf16), shaped((tokens, width), bf16),
            shaped(bp.shape, bf16), shaped(cp.shape, bf16),
            shaped((heads, tokens), f32),
        ),
        in_specs=[inv] * 5 + [anyv] * 12,
        out_specs=(inv,) * 9,
        scratch_shapes=[pltpu.VMEM(a.shape, a.dtype) for a in bulk]
        + [
            vm(n, cap, half), vm(n, cap, half), vm(n, cap, half), vm(n, cap, half),
            vm(n, cap, half), vm(n, cap, half), vm(slots, dwidth), vm(slots, dwidth),
            vf(slots, hid), vf(slots, hid), vm(slots, hid), vf(slots, hid),
            vm(slots, hid), vm(slots, hid), vm(slots, half), vm(slots, half), vm(slots, half),
            vm(n, cap, half), vm(n, cap, half), vm(slots, tokens),
            vm(tokens, dwidth), vm(4, tokens, width), vm(4, tokens, dwidth // 4),
            vf(heads, 1, STATE), vf(n, 1, STATE),
            vm(n, slab, STATE), vm(n, slab, STATE), vm(n, slab, STATE), vm(n, slab, STATE),
            vm(n // 4, rows, width), vm(n // 4, rows, width),
            vf(1, STATE), vf(n, 1, STATE),
            vm(width, STATE), vf(tokens, width), vf(tokens, width), vf(tokens, width),
            vf(tokens, width), vf(tokens, groups * STATE),
            vf(groups, per * tokens, tokens), vm(tokens, per * tokens),
            vm(groups, tokens, per * tokens), vm(per * tokens, width // groups),
            vm(per * tokens, width // groups), vm(tokens, width),
            dma((12,)), dma, dma((4,)), dma, dma((4,)), dma, dma((4,)), dma, dma((4,)),
            dma, dma((4,)), dma, dma, dma, dma,
        ]
        + [dma] * 14,
        compiler_params=pltpu.CompilerParams(
            collective_id=1, has_side_effects=True, vmem_limit_bytes=55 * 1024 * 1024
        ),
        name="backward",
    )(cot, choice, weight, logd, gain, *bulk)


def put_out_kernel(*refs):
    count = len(refs) // 2
    sems = refs[-1]
    copies = [
        pltpu.make_async_copy(refs[i], refs[count + i], sems.at[i]) for i in range(count)
    ]
    for c in copies:
        c.start()
    for c in copies:
        c.wait()


def put_out(arrays):
    anyv = pl.BlockSpec(memory_space=pl.ANY)
    return pl.pallas_call(
        put_out_kernel,
        out_shape=tuple(pltpu.HBM(a.shape, a.dtype) for a in arrays),
        in_specs=[pl.BlockSpec(memory_space=pltpu.VMEM)] * len(arrays),
        out_specs=(pl.BlockSpec(memory_space=pltpu.HBM),) * len(arrays),
        scratch_shapes=[pltpu.SemaphoreType.DMA((len(arrays),))],
        compiler_params=pltpu.CompilerParams(vmem_limit_bytes=1024 * 1024),
        name="put_out",
    )(*[pltpu.with_memory_space_constraint(a, pltpu.VMEM) for a in arrays])


def body(
    mixer_output,
    layer_cotangent,
    expert_choice,
    route_weight,
    gate_pre,
    up_pre,
    w_gate,
    w_up,
    w_down,
    w_out,
    norm_gain,
    scan_in,
    gate_in,
    b_proj,
    c_proj,
    log_decay,
    entry_state,
):
    outs = whole(
        layer_cotangent, expert_choice.T, route_weight.T, log_decay.T, norm_gain[None],
        mixer_output, gate_pre[0], up_pre[0], w_down[0], w_gate[0], w_up[0], w_out,
        scan_in, gate_in, b_proj, c_proj, entry_state.reshape(-1, STATE),
    )
    grad_w_gate, grad_w_up, grad_w_down, *rest = put_out(outs)
    *rest, grad_log_decay = rest
    return (grad_w_gate[None], grad_w_up[None], grad_w_down[None], *rest, grad_log_decay.T)


def solution(mesh):
    split = Mesh(mesh.devices.reshape(4, 4, 4, mesh.shape["tp"]), ("sp_0", "sp_1", "sp_2", "tp"))
    return jax.shard_map(
        body,
        mesh=split,
        in_specs=(
            P(SP, None),
            P(SP, None),
            P(SP, None),
            P(SP, None),
            P(SP, None, "tp"),
            P(SP, None, "tp"),
            P(SP, None, "tp"),
            P(SP, None, "tp"),
            P(SP, "tp", None),
            P("tp", None),
            P("tp"),
            P(SP, "tp"),
            P(SP, "tp"),
            P(SP, "tp"),
            P(SP, "tp"),
            P(SP, "tp"),
            P(SP, "tp", None, None),
        ),
        out_specs=(
            P(SP, None, "tp"),
            P(SP, None, "tp"),
            P(SP, "tp", None),
            P(SP, "tp"),
            P(SP, "tp"),
            P(SP, "tp"),
            P(SP, "tp"),
            P(SP, "tp"),
            P(SP, "tp"),
        ),
        check_vma=False,
    )
```

```python
import jax
import jax.numpy as jnp
from jax import lax
from jax.experimental import pallas as pl
from jax.experimental.pallas import tpu as pltpu
from jax.sharding import Mesh
from jax.sharding import PartitionSpec as P

HEAD_DIM = 64
STATE = 128
SP = ("sp_0", "sp_1", "sp_2")


rms_epsilon = 1e-05
clamp_limit = 7.0
swish_alpha = 1.702


f32, bf16 = jnp.float32, jnp.bfloat16
MESH_ID = pl.DeviceIdType.MESH
NT = (((1,), (1,)), ((), ()))
NN = (((1,), (0,)), ((), ()))
TN = (((0,), (0,)), ((), ()))


def dotf(a, b, dims=NN):
    return lax.dot_general(a, b, dims, preferred_element_type=f32)


def place():
    z, y, x = (lax.axis_index(a) for a in SP)
    return z, y, x, z * 16 + y * 4 + x


def peer_of(k):
    z, y, x, _ = place()
    pz = lax.rem(z + k // 16, 4)
    py = lax.rem(y + lax.rem(k // 4, 4), 4)
    px = lax.rem(x + lax.rem(k, 4), 4)
    return {SP[0]: pz, SP[1]: py, SP[2]: px}, pz * 16 + py * 4 + px


def greet(others):
    barrier = pltpu.get_barrier_semaphore()

    def one(k, _):
        device, _i = peer_of(k)
        pl.semaphore_signal(barrier, inc=1, device_id=device, device_id_type=MESH_ID)
        return 0

    lax.fori_loop(1, others, one, 0)
    partner = {"tp": 1 - lax.axis_index("tp")}
    pl.semaphore_signal(barrier, inc=1, device_id=partner, device_id_type=MESH_ID)


def greeted(others):
    pl.semaphore_wait(pltpu.get_barrier_semaphore(), others)


def push(src, dst, send, recv, device):
    pltpu.make_async_remote_copy(
        src_ref=src, dst_ref=dst, send_sem=send, recv_sem=recv,
        device_id=device, device_id_type=MESH_ID,
    ).start()


def took(ref, sem):
    pltpu.make_async_copy(ref, ref, sem).wait()


HIGH = lax.Precision.HIGHEST
EARLY = 1
MIX = 0
REST = 0
COLL = 1


def exact(a, b, dims=NN):
    return lax.dot_general(a, b, dims, precision=HIGH, preferred_element_type=f32)


def whole_kernel(
    cot, choice, weight, logd, gain,
    mixer_h, gate_h, up_h, wd_h, wg_h, wu_h, wout_h, xin_h, gin_h, bp_h, cp_h, state_h,
    gwg, gwu, gwd, gop_o, gsi_o, ggi_o, gb_o, gc_o, gld_o,
    mixer, gate, up, wd, wg, wu, wout, xin, gin, bp, cp, state,
    send_g, send_h, recv_g, recv_h, oth_g, oth_h, grads, hidden,
    fu, fg, act, acc, gg, ug, psend, precv, pown, rsend, rrecv, hot,
    gh, mixl, coll, dsend, drecv, bsend, brecv, lsend, lrecv, osend, orecv, tsend, trecv,
    stb, so, unit, gy, gxi, gbi, dec, mw, mwt, xm, gym, grown,
    wsem, sg, rg, sh, rh, dsg, drg, dsh, drh, dsp, drp, sr, rr, dso, drout,
    msn, mrv, csn, crv, dsn, drv, bsn, brv, lsn, lrv, osn, orv, tsn, trv, cfw,
):
    n, cap, half = recv_g.shape
    tokens = cot.shape[0]
    z, y, x, me = place()
    plane_at = y * 4 + x
    tp = lax.axis_index("tp")
    partner = {"tp": 1 - tp}
    mine = pl.ds(pl.multiple_of(tp * half, half), half)
    theirs = pl.ds(pl.multiple_of((1 - tp) * half, half), half)
    most = pl.ds(0, n - 1)
    greet(n)
    order = (
        (xin_h, xin), (gin_h, gin), (bp_h, bp), (cp_h, cp), (state_h, state), (mixer_h, mixer),
        (gate_h, gate), (up_h, up), (wd_h, wd), (wg_h, wg), (wu_h, wu), (wout_h, wout),
    )
    loads = [pltpu.make_async_copy(a, b, wsem.at[i]) for i, (a, b) in enumerate(order)]
    for c in loads:
        c.start()

    ti = lax.broadcasted_iota(jnp.int32, (tokens, tokens), 0)
    si = lax.broadcasted_iota(jnp.int32, (tokens, tokens), 1)
    lower = ti >= si
    upper = ti <= si
    experts = lax.broadcasted_iota(jnp.int32, (n, tokens), 0)
    hits = [experts == choice[k : k + 1, :] for k in range(2)]
    named = jnp.where(hits[0] | hits[1], 1.0, 0.0).astype(bf16)
    before = jnp.where(ti < si, 1.0, 0.0).astype(bf16)
    earlier = dotf(named, before)
    places = lax.broadcasted_iota(jnp.int32, (n * cap, tokens), 0)
    hots = []
    for k in range(2):
        rank = jnp.sum(jnp.where(hits[k], earlier, 0.0), axis=0, keepdims=True)
        slot = choice[k : k + 1, :] * cap + rank.astype(jnp.int32)
        hots.append(jnp.where(places == slot, 1.0, 0.0).astype(bf16))
    hot[...] = hots[0] + hots[1]
    weights = exact(jnp.where(ti == si, 1.0, 0.0), weight[...], NT)
    cot_half = cot[:, mine].astype(f32)
    rows0 = (weights[:, 0:1] * cot_half).astype(bf16)
    rows1 = (weights[:, 1:2] * cot_half).astype(bf16)
    packed = dotf(hots[0], rows0) + dotf(hots[1], rows1)
    send_g[...] = packed.reshape(n, cap, half).astype(bf16)
    greeted(n)

    def sends(src, dst, send, recv, first, last):
        def one(k, _):
            device, i = peer_of(k)
            push(src.at[i], dst.at[me], send, recv, device)
            return 0

        lax.fori_loop(first, last, one, 0)

    pltpu.make_async_copy(send_g.at[me], recv_g.at[me], rg.at[z]).start()
    sends(send_g, recv_g, sg, rg.at[z], 1, n)

    heads = logd.shape[0]
    groups = bp.shape[1] // STATE
    width = xin.shape[1]
    per = heads // groups
    gw_cols = width // groups
    ones_low = jnp.where(lower, 1.0, 0.0)
    ones_up = jnp.where(upper, 1.0, 0.0)
    cum = exact(ones_low, logd[...], NT)
    cum_t = exact(logd[...], ones_up)
    growth = jnp.exp(cum)
    tail = jnp.exp(cum[tokens - 1 : tokens, :] - cum)
    lane_head = lax.broadcasted_iota(jnp.int32, (tokens, gw_cols), 1) // HEAD_DIM
    masks = [lane_head == r for r in range(per)]
    for h in range(heads):
        dsend[h] = jnp.broadcast_to(growth[tokens - 1 : tokens, h : h + 1], dsend.shape[1:])
    each = n // heads
    pltpu.make_async_copy(dsend.at[me // each], drecv.at[me], drv).start()

    def send_decay(k, _):
        device, j = peer_of(k)
        push(dsend.at[j // each], drecv.at[me], dsn, drv, device)
        return 0


    def spread(v, g):
        w = jnp.broadcast_to(v[:, g * per : g * per + 1], (tokens, gw_cols))
        for r in range(1, per):
            w = jnp.where(masks[r], v[:, g * per + r : g * per + r + 1], w)
        return w

    def cols(g):
        return slice(g * gw_cols, (g + 1) * gw_cols)

    def states(g):
        return slice(g * STATE, (g + 1) * STATE)

    for c in loads[:5]:
        c.wait()
    invs = []
    for g in range(groups):
        c, b = cp[:, states(g)], bp[:, states(g)]
        inner, inner_t = dotf(c, b, NT), dotf(b, c, NT)
        xg = xin[:, cols(g)]
        for r in range(per):
            h = g * per + r
            col, row = cum[:, h : h + 1], cum_t[h : h + 1, :]
            d = jnp.exp(jnp.where(lower, col - row, -1e30))
            dt = jnp.exp(jnp.where(upper, row - col, -1e30))
            span = slice(r * tokens, (r + 1) * tokens)
            dec[g, span, :] = d
            mw[:, span] = (inner * d).astype(bf16)
            mwt[g, :, span] = (inner_t * dt).astype(bf16)
            xm[span, :] = jnp.where(masks[r], xg.astype(f32), 0.0).astype(bf16)
        stb[cols(g), :] = state[cols(g), :].astype(bf16)
        carry = dotf(c, stb[cols(g), :], NT)
        out = dotf(mw[...], xm[...]) + carry * spread(growth, g)
        so[:, cols(g)] = out
        gf = gin[:, cols(g)].astype(f32)
        gated = out * (gf * jax.nn.sigmoid(gf))
        inv = lax.rsqrt(jnp.mean(gated * gated, axis=1, keepdims=True) + rms_epsilon)
        invs.append(inv)
        u = gated * inv
        unit[:, cols(g)] = u
        mixl[z, :, cols(g)] = (u * gain[:, cols(g)].astype(f32)).astype(bf16)

    def send_mixed():
        for k in range(1, 4):
            push(mixl.at[z], mixl.at[z], msn, mrv, {SP[0]: lax.rem(z + k, 4)})

    if MIX == 0:
        send_mixed()

    loads[5].wait()
    packed = dotf(hot[...], mixer[:, mine])
    send_h[...] = packed.reshape(n, cap, half).astype(bf16)
    pltpu.make_async_copy(send_h.at[me], recv_h.at[me], rh.at[z]).start()

    loads[6].wait()
    loads[7].wait()

    def prepare(i, _):
        rows = pl.ds(pl.multiple_of(i * 64, 64), 64)
        gate_full = gate[rows, :].astype(f32)
        up_full = up[rows, :].astype(f32)
        gate_clip = jnp.minimum(gate_full, clamp_limit)
        up_clip = jnp.clip(up_full, -clamp_limit, clamp_limit)
        sig = jax.nn.sigmoid(swish_alpha * gate_clip)
        swish = gate_clip * sig
        act[rows, :] = ((up_clip + 1.0) * swish).astype(bf16)
        inside = (up_full > -clamp_limit) & (up_full < clamp_limit)
        fu[rows, :] = jnp.where(inside, swish, 0.0)
        slope = sig + swish_alpha * gate_clip * sig * (1.0 - sig)
        fg[rows, :] = jnp.where(gate_full < clamp_limit, (up_clip + 1.0) * slope, 0.0)
        return 0

    lax.fori_loop(0, gate.shape[0] // 64, prepare, 0)
    for c in loads[8:11]:
        c.wait()

    quart = n // 4
    rowsof = quart * cap

    def plane(i):
        q = lax.rem(z - i + 4, 4)
        blocks = pl.ds(pl.multiple_of(q * quart, quart), quart)
        return q, blocks, pl.ds(pl.multiple_of(q * rowsof, rowsof), rowsof)

    def flat(ref, blocks):
        return ref[blocks].astype(f32).reshape(rowsof, half).astype(bf16)

    def arrive(i, _):
        q, blocks, rows = plane(i)
        took(recv_g.at[blocks], rg.at[q])
        push(recv_g.at[blocks], oth_g.at[blocks], dsg, drg.at[q], partner)
        g = flat(recv_g, blocks)
        grads[rows, mine] = g
        acc[rows, :] = dotf(g, wd[:, mine], NT)
        return 0


    def expert(i, _):
        q, blocks, rows = plane(i)
        took(oth_g.at[blocks], drg.at[q])
        g = flat(oth_g, blocks)
        grads[rows, theirs] = g
        act_grad = acc[rows, :] + dotf(g, wd[:, theirs], NT)
        up_grad = (act_grad * fu[rows, :]).astype(bf16)
        gate_grad = (act_grad * fg[rows, :]).astype(bf16)
        ug[rows, :] = up_grad
        gg[rows, :] = gate_grad
        part = dotf(gate_grad, wg[theirs, :], NT) + dotf(up_grad, wu[theirs, :], NT)
        psend[rows, :] = part.astype(bf16)
        push(psend.at[rows], precv.at[rows], dsp, drp.at[q], partner)
        part = dotf(gate_grad, wg[mine, :], NT) + dotf(up_grad, wu[mine, :], NT)
        pown[rows, :] = part.astype(bf16)
        return 0


    def give_back(i, _):
        q, blocks, rows = plane(i)
        took(precv.at[rows], drp.at[q])
        total = pown[rows, :].astype(f32) + precv[rows, :].astype(f32)
        rsend[blocks] = total.reshape(quart, cap, half).astype(bf16)

        def one(k, _):
            device, j = peer_of((4 - i) % 4 * quart + k)
            push(rsend.at[j], rrecv.at[me], sr, rr, device)
            return 0

        lax.fori_loop(1 if i == 0 else 0, quart, one, 0)
        return 0

    arrive(0, 0)
    expert(0, 0)
    give_back(0, 0)
    arrive(1, 0)
    arrive(2, 0)
    expert(1, 0)
    arrive(3, 0)
    sends(send_h, recv_h, sh, rh.at[z], 1, max(1, EARLY * n // 4))
    expert(2, 0)
    give_back(1, 0)
    expert(3, 0)
    give_back(2, 0)
    give_back(3, 0)
    def send_rest(at):
        if REST == at:
            sends(send_h, recv_h, sh, rh.at[z], max(1, EARLY * n // 4), n)

    send_rest(0)
    pltpu.make_async_copy(rsend.at[me], rrecv.at[me], rr).start()

    def down(i, _):
        cols = pl.ds(pl.multiple_of(i * 512, 512), 512)
        gwd[:, cols] = dotf(act[...], grads[:, cols], TN).astype(bf16)
        return 0

    lax.fori_loop(0, grads.shape[1] // 512, down, 0)

    loads[11].wait()
    took(rrecv, rr)
    r = rrecv[...].astype(f32).reshape(n * cap, half).astype(bf16)
    gh[:, mine] = (cot[:, mine].astype(f32) + dotf(hot[...], r, TN)).astype(bf16)
    push(gh.at[:, mine], gh.at[:, mine], dso, drout, partner)
    lax.fori_loop(1, n, send_decay, 0)
    took(gh.at[:, theirs], drout)
    quarter = gh.shape[1] // 4

    owner = z // 2 == tp

    def send_columns():
        for k in range(2):
            pz = 2 * tp + k
            part = pl.ds(pl.multiple_of(pz * quarter, quarter), quarter)

            @pl.when(pz != z)
            def _():
                push(gh.at[:, part], coll.at[z], csn, crv, {SP[0]: pz})

    if COLL == 0:
        send_columns()

    @pl.when(owner)
    def _():
        coll[z] = gh[:, pl.ds(pl.multiple_of(z * quarter, quarter), quarter)]

    send_rest(1)
    slab = bsend.shape[1]
    slabs = gw_cols // slab
    for g in range(groups):
        c = cp[:, states(g)]
        gain_f = gain[:, cols(g)].astype(f32)
        gu = dotf(gh[...], wout[cols(g), :], NT) * gain_f
        u = unit[:, cols(g)]
        out = so[:, cols(g)]
        dgated = invs[g] * (gu - u * jnp.mean(gu * u, axis=1, keepdims=True))
        gf = gin[:, cols(g)].astype(f32)
        sig = jax.nn.sigmoid(gf)
        ggi_o[:, cols(g)] = (dgated * out * sig * (1.0 + gf * (1.0 - sig))).astype(bf16)
        gyg = dgated * (gf * sig)
        gy[:, cols(g)] = gyg
        gr = (gyg * spread(growth, g)).astype(bf16)
        grown[:, cols(g)] = gr
        bs = dotf(gr, c, TN)
        bsend[g * slabs : (g + 1) * slabs] = bs.reshape(slabs, slab, STATE).astype(bf16)

    def exchange(src, dst, send, recv):
        sends(src, dst, send, recv, 1, n)
        pltpu.make_async_copy(src.at[me], dst.at[me], recv).start()

    exchange(bsend, brecv, bsn, brv)
    if COLL == 1:
        send_columns()
    send_rest(2)
    if MIX == 1:
        send_mixed()

    for g in range(groups):
        c, b = cp[:, states(g)], bp[:, states(g)]
        xg = xin[:, cols(g)]
        gyg = gy[:, cols(g)]
        for r in range(per):
            gym[r * tokens : (r + 1) * tokens, :] = jnp.where(masks[r], gyg, 0.0).astype(bf16)
        pairs = dotf(gym[...], xg, NT) * dec[g]
        gw = pairs[:tokens]
        for r in range(1, per):
            gw = gw + pairs[r * tokens : (r + 1) * tokens]
        gw = gw.astype(bf16)
        gxi[:, cols(g)] = dotf(mwt[g], gym[...])
        gc = dotf(gw, b) + dotf(grown[:, cols(g)], stb[cols(g), :])
        gc_o[:, states(g)] = gc.astype(bf16)
        gbi[:, states(g)] = dotf(gw, c, TN)

    took(brecv, brv)
    took(drecv, drv)

    def step(i, acc):
        j = n - 1 - i
        lsend[j] = acc.reshape(slab, STATE).astype(bf16)
        block = brecv[j].astype(f32).reshape(slab // 8, 8, STATE)
        return acc * drecv[j][None] + block

    lax.fori_loop(0, n, step, jnp.zeros((slab // 8, 8, STATE), f32), unroll=4)
    exchange(lsend, lrecv, lsn, lrv)
    send_rest(3)

    @pl.when(owner)
    def _():
        took(coll.at[pl.ds(0, 3)], crv)
        push(coll, coll, csn, cfw, partner)

    @pl.when(jnp.logical_not(owner))
    def _():
        took(coll, cfw)

    took(mixl.at[pl.ds(0, 3)], mrv)
    rows = osend.shape[1]
    left = coll[...].reshape(4 * tokens, quarter)
    right = mixl[...].reshape(4 * tokens, width)
    osend[...] = dotf(left, right, TN).astype(bf16).reshape(n // 4, rows, width)

    def send_outer(k, _):
        py, px = lax.rem(y + k // 4, 4), lax.rem(x + lax.rem(k, 4), 4)
        push(osend.at[py * 4 + px], orecv.at[plane_at], osn, orv, {SP[1]: py, SP[2]: px})
        return 0

    lax.fori_loop(1, n // 4, send_outer, 0)
    pltpu.make_async_copy(osend.at[plane_at], orecv.at[plane_at], orv).start()

    send_rest(4)

    def arrive_h(i, _):
        q, blocks, rows = plane(i)
        took(recv_h.at[blocks], rh.at[q])
        push(recv_h.at[blocks], oth_h.at[blocks], dsh, drh.at[q], partner)
        hidden[rows, mine] = flat(recv_h, blocks)
        return 0

    lax.fori_loop(0, 4, arrive_h, 0)

    def other_h(i, _):
        q, blocks, rows = plane(i)
        took(oth_h.at[blocks], drh.at[q])
        hidden[rows, theirs] = flat(oth_h, blocks)
        return 0

    lax.fori_loop(0, 4, other_h, 0)

    def wide(i, _):
        cols = pl.ds(pl.multiple_of(i * 512, 512), 512)
        h = hidden[:, cols]
        gwg[cols, :] = dotf(h, gg[...], TN).astype(bf16)
        gwu[cols, :] = dotf(h, ug[...], TN).astype(bf16)
        return 0

    lax.fori_loop(0, hidden.shape[1] // 512, wide, 0)

    took(lrecv, lrv)
    ga = jnp.zeros((tokens, STATE), f32)
    for g in range(groups):
        b = bp[:, states(g)]
        xf = xin[:, cols(g)].astype(f32)
        later = lrecv[g * slabs : (g + 1) * slabs].reshape(gw_cols, STATE)
        tails = spread(tail, g)
        gx = gxi[:, cols(g)] + dotf(b, later, NT) * tails
        gsi_o[:, cols(g)] = gx.astype(bf16)
        sel = jnp.where(
            lax.broadcasted_iota(jnp.int32, (gw_cols, STATE), 0) // HEAD_DIM + g * per
            == lax.broadcasted_iota(jnp.int32, (gw_cols, STATE), 1),
            1.0, 0.0,
        )
        ga = ga + exact(gy[:, cols(g)] * so[:, cols(g)] - xf * gx, sel)
    suffix = exact(ones_up, ga)
    tsend[...] = jnp.broadcast_to(suffix[0:1, :], tsend.shape)

    def send_total(k, _):
        device, _j = peer_of(k)
        push(tsend, trecv.at[me], tsn, trv, device)
        return 0

    lax.fori_loop(1, n, send_total, 0)
    for g in range(groups):
        xf = xin[:, cols(g)].astype(f32)
        later = lrecv[g * slabs : (g + 1) * slabs].reshape(gw_cols, STATE)
        gb = gbi[:, states(g)] + dotf((xf * spread(tail, g)).astype(bf16), later)
        gb_o[:, states(g)] = gb.astype(bf16)
    took(orecv, orv)
    total = orecv[0].astype(f32)
    for k in range(1, n // 4):
        total = total + orecv[k].astype(f32)
    gop_o[...] = total
    took(trecv.at[most], trv)
    after = lax.fori_loop(
        me + 1, n, lambda j, t: t + trecv[j], jnp.zeros(tsend.shape, f32)
    )
    total = suffix + after[0:1, :]
    gld_o[...] = exact(total, jnp.where(ti == si, 1.0, 0.0), TN)[:heads, :]

    @pl.when(owner)
    def _():
        took(coll.at[pl.ds(0, 1)], csn)
        took(coll, csn)

    @pl.when(jnp.logical_not(owner))
    def _():
        took(coll.at[pl.ds(0, 2)], csn)

    took(mixl.at[pl.ds(0, 3)], msn)
    took(drecv.at[most], dsn)
    took(bsend.at[most], bsn)
    took(lsend.at[most], lsn)
    took(osend.at[pl.ds(0, n // 4 - 1)], osn)
    took(trecv.at[most], tsn)
    took(gh.at[:, mine], dso)
    took(send_g.at[most], sg)
    took(send_h.at[most], sh)
    took(rsend.at[most], sr)
    took(recv_g, dsg)
    took(recv_h, dsh)
    took(psend, dsp)


def whole(cot, choice, weight, logd, gain, mixer, gate, up, wd, wg, wu, wout, xin, gin, bp, cp, state):
    n = lax.axis_size(SP)
    tokens, dwidth = cot.shape
    slots, hid = gate.shape
    cap, half = slots // n, dwidth // 2
    width = xin.shape[1]
    heads = logd.shape[0]
    groups = bp.shape[1] // STATE
    per = heads // groups
    slab = heads * HEAD_DIM // n
    rows = dwidth // n
    dma = pltpu.SemaphoreType.DMA
    vm = lambda *s: pltpu.VMEM(s, bf16)
    vf = lambda *s: pltpu.VMEM(s, f32)
    inv = pl.BlockSpec(memory_space=pltpu.VMEM)
    anyv = pl.BlockSpec(memory_space=pl.ANY)
    bulk = (mixer, gate, up, wd, wg, wu, wout, xin, gin, bp, cp, state)
    shaped = lambda s, t: pltpu.VMEM(s, t)
    return pl.pallas_call(
        whole_kernel,
        out_shape=(
            shaped((dwidth, hid), bf16), shaped((dwidth, hid), bf16), shaped((hid, dwidth), bf16),
            shaped((rows, width), f32),
            shaped((tokens, width), bf16), shaped((tokens, width), bf16),
            shaped(bp.shape, bf16), shaped(cp.shape, bf16),
            shaped((heads, tokens), f32),
        ),
        in_specs=[inv] * 5 + [anyv] * 12,
        out_specs=(inv,) * 9,
        scratch_shapes=[pltpu.VMEM(a.shape, a.dtype) for a in bulk]
        + [
            vm(n, cap, half), vm(n, cap, half), vm(n, cap, half), vm(n, cap, half),
            vm(n, cap, half), vm(n, cap, half), vm(slots, dwidth), vm(slots, dwidth),
            vf(slots, hid), vf(slots, hid), vm(slots, hid), vf(slots, hid),
            vm(slots, hid), vm(slots, hid), vm(slots, half), vm(slots, half), vm(slots, half),
            vm(n, cap, half), vm(n, cap, half), vm(slots, tokens),
            vm(tokens, dwidth), vm(4, tokens, width), vm(4, tokens, dwidth // 4),
            vf(heads, 1, STATE), vf(n, 1, STATE),
            vm(n, slab, STATE), vm(n, slab, STATE), vm(n, slab, STATE), vm(n, slab, STATE),
            vm(n // 4, rows, width), vm(n // 4, rows, width),
            vf(1, STATE), vf(n, 1, STATE),
            vm(width, STATE), vf(tokens, width), vf(tokens, width), vf(tokens, width),
            vf(tokens, width), vf(tokens, groups * STATE),
            vf(groups, per * tokens, tokens), vm(tokens, per * tokens),
            vm(groups, tokens, per * tokens), vm(per * tokens, width // groups),
            vm(per * tokens, width // groups), vm(tokens, width),
            dma((12,)), dma, dma((4,)), dma, dma((4,)), dma, dma((4,)), dma, dma((4,)),
            dma, dma((4,)), dma, dma, dma, dma,
        ]
        + [dma] * 15,
        compiler_params=pltpu.CompilerParams(
            collective_id=1, has_side_effects=True, vmem_limit_bytes=55 * 1024 * 1024
        ),
        name="backward",
    )(cot, choice, weight, logd, gain, *bulk)


def put_out_kernel(*refs):
    count = len(refs) // 2
    sems = refs[-1]
    copies = [
        pltpu.make_async_copy(refs[i], refs[count + i], sems.at[i]) for i in range(count)
    ]
    for c in copies:
        c.start()
    for c in copies:
        c.wait()


def put_out(arrays):
    anyv = pl.BlockSpec(memory_space=pl.ANY)
    return pl.pallas_call(
        put_out_kernel,
        out_shape=tuple(pltpu.HBM(a.shape, a.dtype) for a in arrays),
        in_specs=[pl.BlockSpec(memory_space=pltpu.VMEM)] * len(arrays),
        out_specs=(pl.BlockSpec(memory_space=pltpu.HBM),) * len(arrays),
        scratch_shapes=[pltpu.SemaphoreType.DMA((len(arrays),))],
        compiler_params=pltpu.CompilerParams(vmem_limit_bytes=1024 * 1024),
        name="put_out",
    )(*[pltpu.with_memory_space_constraint(a, pltpu.VMEM) for a in arrays])


def body(
    mixer_output,
    layer_cotangent,
    expert_choice,
    route_weight,
    gate_pre,
    up_pre,
    w_gate,
    w_up,
    w_down,
    w_out,
    norm_gain,
    scan_in,
    gate_in,
    b_proj,
    c_proj,
    log_decay,
    entry_state,
):
    outs = whole(
        layer_cotangent, expert_choice.T, route_weight.T, log_decay.T, norm_gain[None],
        mixer_output, gate_pre[0], up_pre[0], w_down[0], w_gate[0], w_up[0], w_out,
        scan_in, gate_in, b_proj, c_proj, entry_state.reshape(-1, STATE),
    )
    grad_w_gate, grad_w_up, grad_w_down, *rest = put_out(outs)
    *rest, grad_log_decay = rest
    return (grad_w_gate[None], grad_w_up[None], grad_w_down[None], *rest, grad_log_decay.T)


def solution(mesh):
    split = Mesh(mesh.devices.reshape(4, 4, 4, mesh.shape["tp"]), ("sp_0", "sp_1", "sp_2", "tp"))
    return jax.shard_map(
        body,
        mesh=split,
        in_specs=(
            P(SP, None),
            P(SP, None),
            P(SP, None),
            P(SP, None),
            P(SP, None, "tp"),
            P(SP, None, "tp"),
            P(SP, None, "tp"),
            P(SP, None, "tp"),
            P(SP, "tp", None),
            P("tp", None),
            P("tp"),
            P(SP, "tp"),
            P(SP, "tp"),
            P(SP, "tp"),
            P(SP, "tp"),
            P(SP, "tp"),
            P(SP, "tp", None, None),
        ),
        out_specs=(
            P(SP, None, "tp"),
            P(SP, None, "tp"),
            P(SP, "tp", None),
            P(SP, "tp"),
            P(SP, "tp"),
            P(SP, "tp"),
            P(SP, "tp"),
            P(SP, "tp"),
            P(SP, "tp"),
        ),
        check_vma=False,
    )
```

```python
import jax
import jax.numpy as jnp
from jax import lax
from jax.experimental import pallas as pl
from jax.experimental.pallas import tpu as pltpu
from jax.sharding import Mesh
from jax.sharding import PartitionSpec as P

HEAD_DIM = 64
STATE = 128
SP = ("sp_0", "sp_1", "sp_2")


rms_epsilon = 1e-05
clamp_limit = 7.0
swish_alpha = 1.702


f32, bf16 = jnp.float32, jnp.bfloat16
MESH_ID = pl.DeviceIdType.MESH
NT = (((1,), (1,)), ((), ()))
NN = (((1,), (0,)), ((), ()))
TN = (((0,), (0,)), ((), ()))


def dotf(a, b, dims=NN):
    return lax.dot_general(a, b, dims, preferred_element_type=f32)


def place():
    z, y, x = (lax.axis_index(a) for a in SP)
    return z, y, x, z * 16 + y * 4 + x


def peer_of(k):
    z, y, x, _ = place()
    pz = lax.rem(z + k // 16, 4)
    py = lax.rem(y + lax.rem(k // 4, 4), 4)
    px = lax.rem(x + lax.rem(k, 4), 4)
    return {SP[0]: pz, SP[1]: py, SP[2]: px}, pz * 16 + py * 4 + px


def greet(others):
    barrier = pltpu.get_barrier_semaphore()

    def one(k, _):
        device, _i = peer_of(k)
        pl.semaphore_signal(barrier, inc=1, device_id=device, device_id_type=MESH_ID)
        return 0

    lax.fori_loop(1, others, one, 0)
    partner = {"tp": 1 - lax.axis_index("tp")}
    pl.semaphore_signal(barrier, inc=1, device_id=partner, device_id_type=MESH_ID)


def greeted(others):
    pl.semaphore_wait(pltpu.get_barrier_semaphore(), others)


def push(src, dst, send, recv, device):
    pltpu.make_async_remote_copy(
        src_ref=src, dst_ref=dst, send_sem=send, recv_sem=recv,
        device_id=device, device_id_type=MESH_ID,
    ).start()


def took(ref, sem):
    pltpu.make_async_copy(ref, ref, sem).wait()


HIGH = lax.Precision.HIGHEST
EARLY = 1
MIX = 0
REST = 0
COLL = 1


def exact(a, b, dims=NN):
    return lax.dot_general(a, b, dims, precision=HIGH, preferred_element_type=f32)


def whole_kernel(
    cot, choice, weight, logd, gain,
    mixer_h, gate_h, up_h, wd_h, wg_h, wu_h, wout_h, xin_h, gin_h, bp_h, cp_h, state_h,
    gwg, gwu, gwd, gop_o, gsi_o, ggi_o, gb_o, gc_o, gld_o,
    mixer, gate, up, wd, wg, wu, wout, xin, gin, bp, cp, state,
    send_g, send_h, recv_g, recv_h, oth_g, oth_h, grads, hidden,
    fu, fg, act, acc, gg, ug, psend, precv, pown, rsend, rrecv, hot,
    gh, mixl, coll, dsend, drecv, bsend, brecv, lsend, lrecv, osend, orecv, tsend, trecv,
    stb, so, unit, gy, gxi, gbi, dec, mw, mwt, xm, gym, grown,
    wsem, sg, rg, sh, rh, dsg, drg, dsh, drh, dsp, drp, sr, rr, dso, drout,
    msn, mrv, csn, crv, dsn, drv, bsn, brv, lsn, lrv, osn, orv, tsn, trv, cfw,
):
    n, cap, half = recv_g.shape
    tokens = cot.shape[0]
    z, y, x, me = place()
    plane_at = y * 4 + x
    tp = lax.axis_index("tp")
    partner = {"tp": 1 - tp}
    mine = pl.ds(pl.multiple_of(tp * half, half), half)
    theirs = pl.ds(pl.multiple_of((1 - tp) * half, half), half)
    most = pl.ds(0, n - 1)
    greet(n)
    order = (
        (xin_h, xin), (gin_h, gin), (bp_h, bp), (cp_h, cp), (state_h, state), (mixer_h, mixer),
        (gate_h, gate), (up_h, up), (wd_h, wd), (wg_h, wg), (wu_h, wu), (wout_h, wout),
    )
    loads = [pltpu.make_async_copy(a, b, wsem.at[i]) for i, (a, b) in enumerate(order)]
    for c in loads:
        c.start()

    ti = lax.broadcasted_iota(jnp.int32, (tokens, tokens), 0)
    si = lax.broadcasted_iota(jnp.int32, (tokens, tokens), 1)
    lower = ti >= si
    upper = ti <= si
    experts = lax.broadcasted_iota(jnp.int32, (n, tokens), 0)
    hits = [experts == choice[k : k + 1, :] for k in range(2)]
    named = jnp.where(hits[0] | hits[1], 1.0, 0.0).astype(bf16)
    before = jnp.where(ti < si, 1.0, 0.0).astype(bf16)
    earlier = dotf(named, before)
    places = lax.broadcasted_iota(jnp.int32, (n * cap, tokens), 0)
    hots = []
    for k in range(2):
        rank = jnp.sum(jnp.where(hits[k], earlier, 0.0), axis=0, keepdims=True)
        slot = choice[k : k + 1, :] * cap + rank.astype(jnp.int32)
        hots.append(jnp.where(places == slot, 1.0, 0.0).astype(bf16))
    hot[...] = hots[0] + hots[1]
    weights = exact(jnp.where(ti == si, 1.0, 0.0), weight[...], NT)
    cot_half = cot[:, mine].astype(f32)
    rows0 = (weights[:, 0:1] * cot_half).astype(bf16)
    rows1 = (weights[:, 1:2] * cot_half).astype(bf16)
    packed = dotf(hots[0], rows0) + dotf(hots[1], rows1)
    send_g[...] = packed.reshape(n, cap, half).astype(bf16)
    greeted(n)

    def sends(src, dst, send, recv, first, last):
        def one(k, _):
            device, i = peer_of(k)
            push(src.at[i], dst.at[me], send, recv, device)
            return 0

        lax.fori_loop(first, last, one, 0)

    pltpu.make_async_copy(send_g.at[me], recv_g.at[me], rg.at[z]).start()
    sends(send_g, recv_g, sg, rg.at[z], 1, n)

    heads = logd.shape[0]
    groups = bp.shape[1] // STATE
    width = xin.shape[1]
    per = heads // groups
    gw_cols = width // groups
    ones_low = jnp.where(lower, 1.0, 0.0)
    ones_up = jnp.where(upper, 1.0, 0.0)
    cum = exact(ones_low, logd[...], NT)
    cum_t = exact(logd[...], ones_up)
    growth = jnp.exp(cum)
    tail = jnp.exp(cum[tokens - 1 : tokens, :] - cum)
    lane_head = lax.broadcasted_iota(jnp.int32, (tokens, gw_cols), 1) // HEAD_DIM
    masks = [lane_head == r for r in range(per)]
    for h in range(heads):
        dsend[h] = jnp.broadcast_to(growth[tokens - 1 : tokens, h : h + 1], dsend.shape[1:])
    each = n // heads
    pltpu.make_async_copy(dsend.at[me // each], drecv.at[me], drv).start()

    def send_decay(k, _):
        device, j = peer_of(k)
        push(dsend.at[j // each], drecv.at[me], dsn, drv, device)
        return 0


    def spread(v, g):
        w = jnp.broadcast_to(v[:, g * per : g * per + 1], (tokens, gw_cols))
        for r in range(1, per):
            w = jnp.where(masks[r], v[:, g * per + r : g * per + r + 1], w)
        return w

    def cols(g):
        return slice(g * gw_cols, (g + 1) * gw_cols)

    gain_rows = gain[...].astype(f32)
    lines = gw_cols // STATE

    def gains(g):
        at = range(g * lines, (g + 1) * lines)
        return jnp.concatenate([gain_rows[i : i + 1, :] for i in at], axis=1)

    def states(g):
        return slice(g * STATE, (g + 1) * STATE)

    for c in loads[:5]:
        c.wait()
    invs = []
    for g in range(groups):
        c, b = cp[:, states(g)], bp[:, states(g)]
        inner, inner_t = dotf(c, b, NT), dotf(b, c, NT)
        xg = xin[:, cols(g)]
        for r in range(per):
            h = g * per + r
            col, row = cum[:, h : h + 1], cum_t[h : h + 1, :]
            d = jnp.exp(jnp.where(lower, col - row, -1e30))
            dt = jnp.exp(jnp.where(upper, row - col, -1e30))
            span = slice(r * tokens, (r + 1) * tokens)
            dec[g, span, :] = d
            mw[:, span] = (inner * d).astype(bf16)
            mwt[g, :, span] = (inner_t * dt).astype(bf16)
            xm[span, :] = jnp.where(masks[r], xg.astype(f32), 0.0).astype(bf16)
        stb[cols(g), :] = state[cols(g), :].astype(bf16)
        carry = dotf(c, stb[cols(g), :], NT)
        out = dotf(mw[...], xm[...]) + carry * spread(growth, g)
        so[:, cols(g)] = out
        gf = gin[:, cols(g)].astype(f32)
        gated = out * (gf * jax.nn.sigmoid(gf))
        inv = lax.rsqrt(jnp.mean(gated * gated, axis=1, keepdims=True) + rms_epsilon)
        invs.append(inv)
        u = gated * inv
        unit[:, cols(g)] = u
        mixl[z, :, cols(g)] = (u * gains(g)).astype(bf16)

    def send_mixed():
        for k in range(1, 4):
            push(mixl.at[z], mixl.at[z], msn, mrv, {SP[0]: lax.rem(z + k, 4)})

    if MIX == 0:
        send_mixed()

    loads[5].wait()
    packed = dotf(hot[...], mixer[:, mine])
    send_h[...] = packed.reshape(n, cap, half).astype(bf16)
    pltpu.make_async_copy(send_h.at[me], recv_h.at[me], rh.at[z]).start()

    loads[6].wait()
    loads[7].wait()

    def prepare(i, _):
        rows = pl.ds(pl.multiple_of(i * 64, 64), 64)
        gate_full = gate[rows, :].astype(f32)
        up_full = up[rows, :].astype(f32)
        gate_clip = jnp.minimum(gate_full, clamp_limit)
        up_clip = jnp.clip(up_full, -clamp_limit, clamp_limit)
        sig = jax.nn.sigmoid(swish_alpha * gate_clip)
        swish = gate_clip * sig
        act[rows, :] = ((up_clip + 1.0) * swish).astype(bf16)
        inside = (up_full > -clamp_limit) & (up_full < clamp_limit)
        fu[rows, :] = jnp.where(inside, swish, 0.0)
        slope = sig + swish_alpha * gate_clip * sig * (1.0 - sig)
        fg[rows, :] = jnp.where(gate_full < clamp_limit, (up_clip + 1.0) * slope, 0.0)
        return 0

    lax.fori_loop(0, gate.shape[0] // 64, prepare, 0)
    for c in loads[8:11]:
        c.wait()

    quart = n // 4
    rowsof = quart * cap

    def plane(i):
        q = lax.rem(z - i + 4, 4)
        blocks = pl.ds(pl.multiple_of(q * quart, quart), quart)
        return q, blocks, pl.ds(pl.multiple_of(q * rowsof, rowsof), rowsof)

    def flat(ref, blocks):
        return ref[blocks].astype(f32).reshape(rowsof, half).astype(bf16)

    def arrive(i, _):
        q, blocks, rows = plane(i)
        took(recv_g.at[blocks], rg.at[q])
        push(recv_g.at[blocks], oth_g.at[blocks], dsg, drg.at[q], partner)
        g = flat(recv_g, blocks)
        grads[rows, mine] = g
        acc[rows, :] = dotf(g, wd[:, mine], NT)
        return 0


    def expert(i, _):
        q, blocks, rows = plane(i)
        took(oth_g.at[blocks], drg.at[q])
        g = flat(oth_g, blocks)
        grads[rows, theirs] = g
        act_grad = acc[rows, :] + dotf(g, wd[:, theirs], NT)
        up_grad = (act_grad * fu[rows, :]).astype(bf16)
        gate_grad = (act_grad * fg[rows, :]).astype(bf16)
        ug[rows, :] = up_grad
        gg[rows, :] = gate_grad
        part = dotf(gate_grad, wg[theirs, :], NT) + dotf(up_grad, wu[theirs, :], NT)
        psend[rows, :] = part.astype(bf16)
        push(psend.at[rows], precv.at[rows], dsp, drp.at[q], partner)
        part = dotf(gate_grad, wg[mine, :], NT) + dotf(up_grad, wu[mine, :], NT)
        pown[rows, :] = part.astype(bf16)
        return 0


    def give_back(i, _):
        q, blocks, rows = plane(i)
        took(precv.at[rows], drp.at[q])
        total = pown[rows, :].astype(f32) + precv[rows, :].astype(f32)
        rsend[blocks] = total.reshape(quart, cap, half).astype(bf16)

        def one(k, _):
            device, j = peer_of((4 - i) % 4 * quart + k)
            push(rsend.at[j], rrecv.at[me], sr, rr, device)
            return 0

        lax.fori_loop(1 if i == 0 else 0, quart, one, 0)
        return 0

    arrive(0, 0)
    expert(0, 0)
    give_back(0, 0)
    arrive(1, 0)
    arrive(2, 0)
    expert(1, 0)
    arrive(3, 0)
    sends(send_h, recv_h, sh, rh.at[z], 1, max(1, EARLY * n // 4))
    expert(2, 0)
    give_back(1, 0)
    expert(3, 0)
    give_back(2, 0)
    give_back(3, 0)
    def send_rest(at):
        if REST == at:
            sends(send_h, recv_h, sh, rh.at[z], max(1, EARLY * n // 4), n)

    send_rest(0)
    pltpu.make_async_copy(rsend.at[me], rrecv.at[me], rr).start()

    def down(i, _):
        cols = pl.ds(pl.multiple_of(i * 512, 512), 512)
        gwd[:, cols] = dotf(act[...], grads[:, cols], TN).astype(bf16)
        return 0

    lax.fori_loop(0, grads.shape[1] // 512, down, 0)

    loads[11].wait()
    took(rrecv, rr)
    r = rrecv[...].astype(f32).reshape(n * cap, half).astype(bf16)
    gh[:, mine] = (cot[:, mine].astype(f32) + dotf(hot[...], r, TN)).astype(bf16)
    push(gh.at[:, mine], gh.at[:, mine], dso, drout, partner)
    lax.fori_loop(1, n, send_decay, 0)
    took(gh.at[:, theirs], drout)
    quarter = gh.shape[1] // 4

    owner = z // 2 == tp

    def send_columns():
        for k in range(2):
            pz = 2 * tp + k
            part = pl.ds(pl.multiple_of(pz * quarter, quarter), quarter)

            @pl.when(pz != z)
            def _():
                push(gh.at[:, part], coll.at[z], csn, crv, {SP[0]: pz})

    if COLL == 0:
        send_columns()

    @pl.when(owner)
    def _():
        coll[z] = gh[:, pl.ds(pl.multiple_of(z * quarter, quarter), quarter)]

    send_rest(1)
    slab = bsend.shape[1]
    slabs = gw_cols // slab
    for g in range(groups):
        c = cp[:, states(g)]
        gain_f = gains(g)
        gu = dotf(gh[...], wout[cols(g), :], NT) * gain_f
        u = unit[:, cols(g)]
        out = so[:, cols(g)]
        dgated = invs[g] * (gu - u * jnp.mean(gu * u, axis=1, keepdims=True))
        gf = gin[:, cols(g)].astype(f32)
        sig = jax.nn.sigmoid(gf)
        ggi_o[:, cols(g)] = (dgated * out * sig * (1.0 + gf * (1.0 - sig))).astype(bf16)
        gyg = dgated * (gf * sig)
        gy[:, cols(g)] = gyg
        gr = (gyg * spread(growth, g)).astype(bf16)
        grown[:, cols(g)] = gr
        bs = dotf(gr, c, TN)
        bsend[g * slabs : (g + 1) * slabs] = bs.reshape(slabs, slab, STATE).astype(bf16)

    def exchange(src, dst, send, recv):
        sends(src, dst, send, recv, 1, n)
        pltpu.make_async_copy(src.at[me], dst.at[me], recv).start()

    exchange(bsend, brecv, bsn, brv)
    if COLL == 1:
        send_columns()
    send_rest(2)
    if MIX == 1:
        send_mixed()

    for g in range(groups):
        c, b = cp[:, states(g)], bp[:, states(g)]
        xg = xin[:, cols(g)]
        gyg = gy[:, cols(g)]
        for r in range(per):
            gym[r * tokens : (r + 1) * tokens, :] = jnp.where(masks[r], gyg, 0.0).astype(bf16)
        pairs = dotf(gym[...], xg, NT) * dec[g]
        gw = pairs[:tokens]
        for r in range(1, per):
            gw = gw + pairs[r * tokens : (r + 1) * tokens]
        gw = gw.astype(bf16)
        gxi[:, cols(g)] = dotf(mwt[g], gym[...])
        gc = dotf(gw, b) + dotf(grown[:, cols(g)], stb[cols(g), :])
        gc_o[:, states(g)] = gc.astype(bf16)
        gbi[:, states(g)] = dotf(gw, c, TN)

    took(brecv, brv)
    took(drecv, drv)

    def step(i, acc):
        j = n - 1 - i
        lsend[j] = acc.reshape(slab, STATE).astype(bf16)
        block = brecv[j].astype(f32).reshape(slab // 8, 8, STATE)
        return acc * drecv[j][None] + block

    lax.fori_loop(0, n, step, jnp.zeros((slab // 8, 8, STATE), f32), unroll=4)
    exchange(lsend, lrecv, lsn, lrv)
    send_rest(3)

    @pl.when(owner)
    def _():
        took(coll.at[pl.ds(0, 3)], crv)
        push(coll, coll, csn, cfw, partner)

    @pl.when(jnp.logical_not(owner))
    def _():
        took(coll, cfw)

    took(mixl.at[pl.ds(0, 3)], mrv)
    rows = osend.shape[1]
    left = coll[...].reshape(4 * tokens, quarter)
    right = mixl[...].reshape(4 * tokens, width)
    osend[...] = dotf(left, right, TN).astype(bf16).reshape(n // 4, rows, width)

    def send_outer(k, _):
        py, px = lax.rem(y + k // 4, 4), lax.rem(x + lax.rem(k, 4), 4)
        push(osend.at[py * 4 + px], orecv.at[plane_at], osn, orv, {SP[1]: py, SP[2]: px})
        return 0

    lax.fori_loop(1, n // 4, send_outer, 0)
    pltpu.make_async_copy(osend.at[plane_at], orecv.at[plane_at], orv).start()

    send_rest(4)

    def arrive_h(i, _):
        q, blocks, rows = plane(i)
        took(recv_h.at[blocks], rh.at[q])
        push(recv_h.at[blocks], oth_h.at[blocks], dsh, drh.at[q], partner)
        hidden[rows, mine] = flat(recv_h, blocks)
        return 0

    lax.fori_loop(0, 4, arrive_h, 0)

    def other_h(i, _):
        q, blocks, rows = plane(i)
        took(oth_h.at[blocks], drh.at[q])
        hidden[rows, theirs] = flat(oth_h, blocks)
        return 0

    lax.fori_loop(0, 4, other_h, 0)

    def wide(i, _):
        cols = pl.ds(pl.multiple_of(i * 512, 512), 512)
        h = hidden[:, cols]
        gwg[cols, :] = dotf(h, gg[...], TN).astype(bf16)
        gwu[cols, :] = dotf(h, ug[...], TN).astype(bf16)
        return 0

    lax.fori_loop(0, hidden.shape[1] // 512, wide, 0)

    took(lrecv, lrv)
    ga = jnp.zeros((tokens, STATE), f32)
    for g in range(groups):
        b = bp[:, states(g)]
        xf = xin[:, cols(g)].astype(f32)
        later = lrecv[g * slabs : (g + 1) * slabs].reshape(gw_cols, STATE)
        tails = spread(tail, g)
        gx = gxi[:, cols(g)] + dotf(b, later, NT) * tails
        gsi_o[:, cols(g)] = gx.astype(bf16)
        sel = jnp.where(
            lax.broadcasted_iota(jnp.int32, (gw_cols, STATE), 0) // HEAD_DIM + g * per
            == lax.broadcasted_iota(jnp.int32, (gw_cols, STATE), 1),
            1.0, 0.0,
        )
        ga = ga + exact(gy[:, cols(g)] * so[:, cols(g)] - xf * gx, sel)
    suffix = exact(ones_up, ga)
    tsend[...] = jnp.broadcast_to(suffix[0:1, :], tsend.shape)

    def send_total(k, _):
        device, _j = peer_of(k)
        push(tsend, trecv.at[me], tsn, trv, device)
        return 0

    lax.fori_loop(1, n, send_total, 0)
    for g in range(groups):
        xf = xin[:, cols(g)].astype(f32)
        later = lrecv[g * slabs : (g + 1) * slabs].reshape(gw_cols, STATE)
        gb = gbi[:, states(g)] + dotf((xf * spread(tail, g)).astype(bf16), later)
        gb_o[:, states(g)] = gb.astype(bf16)
    took(orecv, orv)
    total = orecv[0].astype(f32)
    for k in range(1, n // 4):
        total = total + orecv[k].astype(f32)
    gop_o[...] = total
    took(trecv.at[most], trv)
    after = lax.fori_loop(
        me + 1, n, lambda j, t: t + trecv[j], jnp.zeros(tsend.shape, f32)
    )
    total = suffix + after[0:1, :]
    gld_o[...] = exact(total, jnp.where(ti == si, 1.0, 0.0), TN)[:heads, :]

    @pl.when(owner)
    def _():
        took(coll.at[pl.ds(0, 1)], csn)
        took(coll, csn)

    @pl.when(jnp.logical_not(owner))
    def _():
        took(coll.at[pl.ds(0, 2)], csn)

    took(mixl.at[pl.ds(0, 3)], msn)
    took(drecv.at[most], dsn)
    took(bsend.at[most], bsn)
    took(lsend.at[most], lsn)
    took(osend.at[pl.ds(0, n // 4 - 1)], osn)
    took(trecv.at[most], tsn)
    took(gh.at[:, mine], dso)
    took(send_g.at[most], sg)
    took(send_h.at[most], sh)
    took(rsend.at[most], sr)
    took(recv_g, dsg)
    took(recv_h, dsh)
    took(psend, dsp)


def whole(cot, choice, weight, logd, gain, mixer, gate, up, wd, wg, wu, wout, xin, gin, bp, cp, state):
    n = lax.axis_size(SP)
    tokens, dwidth = cot.shape
    slots, hid = gate.shape
    cap, half = slots // n, dwidth // 2
    width = xin.shape[1]
    heads = logd.shape[0]
    groups = bp.shape[1] // STATE
    per = heads // groups
    slab = heads * HEAD_DIM // n
    rows = dwidth // n
    dma = pltpu.SemaphoreType.DMA
    vm = lambda *s: pltpu.VMEM(s, bf16)
    vf = lambda *s: pltpu.VMEM(s, f32)
    inv = pl.BlockSpec(memory_space=pltpu.VMEM)
    anyv = pl.BlockSpec(memory_space=pl.ANY)
    bulk = (mixer, gate, up, wd, wg, wu, wout, xin, gin, bp, cp, state)
    shaped = lambda s, t: pltpu.VMEM(s, t)
    return pl.pallas_call(
        whole_kernel,
        out_shape=(
            shaped((dwidth, hid), bf16), shaped((dwidth, hid), bf16), shaped((hid, dwidth), bf16),
            shaped((rows, width), f32),
            shaped((tokens, width), bf16), shaped((tokens, width), bf16),
            shaped(bp.shape, bf16), shaped(cp.shape, bf16),
            shaped((heads, tokens), f32),
        ),
        in_specs=[inv] * 5 + [anyv] * 12,
        out_specs=(inv,) * 9,
        scratch_shapes=[pltpu.VMEM(a.shape, a.dtype) for a in bulk]
        + [
            vm(n, cap, half), vm(n, cap, half), vm(n, cap, half), vm(n, cap, half),
            vm(n, cap, half), vm(n, cap, half), vm(slots, dwidth), vm(slots, dwidth),
            vf(slots, hid), vf(slots, hid), vm(slots, hid), vf(slots, hid),
            vm(slots, hid), vm(slots, hid), vm(slots, half), vm(slots, half), vm(slots, half),
            vm(n, cap, half), vm(n, cap, half), vm(slots, tokens),
            vm(tokens, dwidth), vm(4, tokens, width), vm(4, tokens, dwidth // 4),
            vf(heads, 1, STATE), vf(n, 1, STATE),
            vm(n, slab, STATE), vm(n, slab, STATE), vm(n, slab, STATE), vm(n, slab, STATE),
            vm(n // 4, rows, width), vm(n // 4, rows, width),
            vf(1, STATE), vf(n, 1, STATE),
            vm(width, STATE), vf(tokens, width), vf(tokens, width), vf(tokens, width),
            vf(tokens, width), vf(tokens, groups * STATE),
            vf(groups, per * tokens, tokens), vm(tokens, per * tokens),
            vm(groups, tokens, per * tokens), vm(per * tokens, width // groups),
            vm(per * tokens, width // groups), vm(tokens, width),
            dma((12,)), dma, dma((4,)), dma, dma((4,)), dma, dma((4,)), dma, dma((4,)),
            dma, dma((4,)), dma, dma, dma, dma,
        ]
        + [dma] * 15,
        compiler_params=pltpu.CompilerParams(
            collective_id=1, has_side_effects=True, vmem_limit_bytes=55 * 1024 * 1024
        ),
        name="backward",
    )(cot, choice, weight, logd, gain, *bulk)


def put_out_kernel(*refs):
    count = len(refs) // 2
    sems = refs[-1]
    copies = [
        pltpu.make_async_copy(refs[i], refs[count + i], sems.at[i]) for i in range(count)
    ]
    for c in copies:
        c.start()
    for c in copies:
        c.wait()


def put_out(arrays):
    anyv = pl.BlockSpec(memory_space=pl.ANY)
    return pl.pallas_call(
        put_out_kernel,
        out_shape=tuple(pltpu.HBM(a.shape, a.dtype) for a in arrays),
        in_specs=[pl.BlockSpec(memory_space=pltpu.VMEM)] * len(arrays),
        out_specs=(pl.BlockSpec(memory_space=pltpu.HBM),) * len(arrays),
        scratch_shapes=[pltpu.SemaphoreType.DMA((len(arrays),))],
        compiler_params=pltpu.CompilerParams(vmem_limit_bytes=1024 * 1024),
        name="put_out",
    )(*[pltpu.with_memory_space_constraint(a, pltpu.VMEM) for a in arrays])


def body(
    mixer_output,
    layer_cotangent,
    expert_choice,
    route_weight,
    gate_pre,
    up_pre,
    w_gate,
    w_up,
    w_down,
    w_out,
    norm_gain,
    scan_in,
    gate_in,
    b_proj,
    c_proj,
    log_decay,
    entry_state,
):
    outs = whole(
        layer_cotangent, expert_choice.T, route_weight.T, log_decay.T, norm_gain.reshape(-1, STATE),
        mixer_output, gate_pre[0], up_pre[0], w_down[0], w_gate[0], w_up[0], w_out,
        scan_in, gate_in, b_proj, c_proj, entry_state.reshape(-1, STATE),
    )
    grad_w_gate, grad_w_up, grad_w_down, *rest = put_out(outs)
    *rest, grad_log_decay = rest
    return (grad_w_gate[None], grad_w_up[None], grad_w_down[None], *rest, grad_log_decay.T)


def solution(mesh):
    split = Mesh(mesh.devices.reshape(4, 4, 4, mesh.shape["tp"]), ("sp_0", "sp_1", "sp_2", "tp"))
    return jax.shard_map(
        body,
        mesh=split,
        in_specs=(
            P(SP, None),
            P(SP, None),
            P(SP, None),
            P(SP, None),
            P(SP, None, "tp"),
            P(SP, None, "tp"),
            P(SP, None, "tp"),
            P(SP, None, "tp"),
            P(SP, "tp", None),
            P("tp", None),
            P("tp"),
            P(SP, "tp"),
            P(SP, "tp"),
            P(SP, "tp"),
            P(SP, "tp"),
            P(SP, "tp"),
            P(SP, "tp", None, None),
        ),
        out_specs=(
            P(SP, None, "tp"),
            P(SP, None, "tp"),
            P(SP, "tp", None),
            P(SP, "tp"),
            P(SP, "tp"),
            P(SP, "tp"),
            P(SP, "tp"),
            P(SP, "tp"),
            P(SP, "tp"),
        ),
        check_vma=False,
    )
```
